32 devices in a mesh: sp: 4 (over z), fs: 4 (over y, x), tp: 2 (over core).
Axes of the slice: x: 2, y: 2, z: 4, core: 2. Of those that a mesh axis runs over, the one named last changes fastest.
Arguments:
- inputs: bfloat16 [4, 512, 2048], P('fs', 'sp', 'tp'), may hold values from -6 to 6
- input_norm_scale: float32 [2048], replicated, may hold values from 0.1 to 1.9
- query_matrix: bfloat16 [2048, 512], P('sp', 'tp'), may hold values from -0.125 to 0.125
- key_matrix: bfloat16 [2048, 512], P('sp', 'tp'), may hold values from -0.125 to 0.125
- value_matrix: bfloat16 [2048, 512], P('sp', 'tp'), may hold values from -0.125 to 0.125
- decay_down_weight: bfloat16 [2048, 128], replicated, may hold values from -0.125 to 0.125
- decay_up_weight: bfloat16 [128, 512], P(None, 'tp'), may hold values from -1.1953125 to 1.1953125
- decay_bias_base: float32 [512], P('tp'), as said below
- decay_position_offset: float32 [4, 512, 8], P('fs', 'sp', 'tp'), may hold values from -0.7 to 0.7
- extra_log_decay: float32 [4, 512, 8], P('fs', 'sp', 'tp'), may hold values from -2.8 to 0, as said below
- correction_down_weight: bfloat16 [2048, 128], replicated, may hold values from -0.125 to 0.125
- correction_up_weight: bfloat16 [128, 512], P(None, 'tp'), may hold values from -1.1953125 to 1.1953125
- correction_rate_bias: float32 [512], P('tp'), as said below
- head_norm_scale: float32 [512], P('tp'), may hold values from 0.1 to 1.9
- starting_states: float32 [4, 2, 8, 64, 64], P('fs', None, 'tp'), may hold values from -128 to 128
- pointwise_value_weight: bfloat16 [2048, 1024], P('sp', 'tp'), may hold values from -0.125 to 0.125
- pointwise_gate_weight: bfloat16 [2048, 1024], P('sp', 'tp'), may hold values from -0.125 to 0.125
- depthwise_taps_weight: float32 [31, 1024], P(None, 'tp')
- channel_norm_scale: float32 [1024], P('tp'), may hold values from 0.1 to 1.9
- mixer_output_weight: bfloat16 [512, 2048], P('tp', 'sp'), may hold values from -0.15625 to 0.15625
- convolution_output_weight: bfloat16 [1024, 2048], P('tp', 'sp'), may hold values from -0.15625 to 0.15625
Outputs:
- mixed: bfloat16 [4, 512, 2048], P('fs', ('sp', 'tp'))
The draws below stay inside these ranges and needn't reach their ends.
Inputs may be any that keep to these rules, and one draw needn't show every extreme that they name: `decay_bias_base`: decay bases, one value for every channel. `correction_rate_bias`: correction-rate bases, one value for every channel. `extra_log_decay`: zero at all but a few positions of each sequence.
All inputs are finite; a program needn't handle non-finite values.
Results may differ from the reference program's by a relative error of at most 0.012.
Values may be sent and summed in bfloat16 or wider, within the bound.
A program may use at most 64 MiB of HBM per device.

```python
import jax
import jax.numpy as jnp
from jax import lax

D = 2048
ATTN_GROUP_SIZE = 64
RANK = 128
CONV_K = 31
RW_H = 8
TOK_DEV = 128
RW_W = 512
CW = 1024
SEQ_LEN = 512
BATCH = 4


def slow_heads(key):
    order = jax.random.permutation(jax.random.fold_in(key, 11), RW_H)
    return order >= RW_H // 2


def draw_decay_bias_base(key, part):
    slow = jnp.repeat(slow_heads(key), ATTN_GROUP_SIZE)
    jitter = jax.random.uniform(jax.random.fold_in(key, 12), (RW_H * ATTN_GROUP_SIZE,), jnp.float32, -0.5, 0.5)
    slow_value = jnp.log(0.25 / SEQ_LEN) + 0.5
    return jnp.where(slow, slow_value, -3.0) + jitter


def draw_correction_rate_bias(key, part):
    slow = jnp.repeat(slow_heads(key), ATTN_GROUP_SIZE)
    jitter = jax.random.uniform(jax.random.fold_in(key, 13), (RW_H * ATTN_GROUP_SIZE,), jnp.float32, -0.5, 0.5)
    spread = jax.random.uniform(jax.random.fold_in(key, 14), (RW_H * ATTN_GROUP_SIZE,), jnp.float32, -1.0, 1.0)
    return jnp.where(slow, jnp.log(16.0 / SEQ_LEN) + jitter, spread)


def draw_decay_position_offset(key, part):
    blocks = SEQ_LEN // TOK_DEV
    offsets = jax.random.uniform(jax.random.fold_in(key, 15), (BATCH, blocks, RW_H), jnp.float32, -0.7, 0.7)
    return jnp.repeat(offsets, TOK_DEV, axis=1)


def draw_extra_log_decay(key, part):
    places = jax.random.randint(jax.random.fold_in(key, 21), (BATCH, 4), 0, SEQ_LEN)
    losses = jnp.log(jax.random.uniform(jax.random.fold_in(key, 22), (BATCH, 4, RW_H), jnp.float32, 0.5, 0.8))
    hits = (jnp.arange(SEQ_LEN)[None, :, None] == places[:, None, :]).astype(jnp.float32)
    return jnp.einsum('blp,bph->blh', hits, losses)


def draw_depthwise_taps_weight(key, part):
    rising = jnp.exp(jnp.linspace(jnp.log(0.3), jnp.log(3.0), CW))
    values = jax.random.normal(jax.random.fold_in(key, 23), (CONV_K, CW), jnp.float32)
    return values * rising[None, :] / jnp.sqrt(float(CONV_K))


def level_of(rng, dims, shards, smallest, largest):
    loudness = 1.0
    for axis_at, parts in shards:
        draws = jax.random.uniform(jax.random.fold_in(jax.random.fold_in(rng, 6), axis_at), (parts,), jnp.float32, smallest / len(shards), largest / len(shards))
        loudness = loudness * jnp.repeat(jnp.exp(draws), dims[axis_at] // parts).reshape((-1,) + (1,) * (len(dims) - 1 - axis_at))
    return loudness


def normal_values(own_key, extent, scale, most, split=(), kind=jnp.bfloat16):
    result = jax.random.normal(own_key, extent, jnp.float32) * scale
    if len(split) > 0:
        result = level_of(own_key, extent, split, -0.22, 0.18) * result
    return jnp.clip(result, min=-most, max=most).astype(kind)


def setup_inputs(seed: int = 0) -> dict:
    streams_of = jax.random.split(jax.random.key(seed), 22)
    inputs = normal_values(streams_of[0], (BATCH, SEQ_LEN, D), 1.0, 6.0, ((0, 4), (1, 4), (2, 2)))
    input_norm_scale = jnp.clip(1.0 + 0.18 * jax.random.normal(streams_of[1], (D,), jnp.float32), 0.1, 1.9)
    query_matrix = normal_values(streams_of[2], (D, RW_W), D ** -0.5, 0.125, ((0, 4), (1, 2)))
    key_matrix = normal_values(streams_of[3], (D, RW_W), D ** -0.5, 0.125, ((0, 4), (1, 2)))
    value_matrix = normal_values(streams_of[4], (D, RW_W), D ** -0.5, 0.125, ((0, 4), (1, 2)))
    decay_down_weight = normal_values(streams_of[5], (D, RANK), D ** -0.5, 0.125)
    decay_up_weight = normal_values(streams_of[6], (RANK, RW_W), 0.2, 1.1953125, ((1, 2),))
    decay_bias_base = draw_decay_bias_base(jax.random.fold_in(streams_of[21], 71), 0)
    decay_position_offset = draw_decay_position_offset(jax.random.fold_in(streams_of[21], 71), 0)
    extra_log_decay = draw_extra_log_decay(jax.random.fold_in(streams_of[21], 71), 0)
    correction_down_weight = normal_values(streams_of[10], (D, RANK), D ** -0.5, 0.125)
    correction_up_weight = normal_values(streams_of[11], (RANK, RW_W), 0.2, 1.1953125, ((1, 2),))
    correction_rate_bias = draw_correction_rate_bias(jax.random.fold_in(streams_of[21], 71), 0)
    head_norm_scale = jnp.clip(1.0 + 0.18 * jax.random.normal(streams_of[13], (RW_W,), jnp.float32), 0.1, 1.9)
    starting_states = normal_values(streams_of[14], (BATCH, 2, RW_H, ATTN_GROUP_SIZE, ATTN_GROUP_SIZE), (SEQ_LEN ** 0.5), 128.0, ((0, 4), (2, 2)), jnp.float32)
    pointwise_value_weight = normal_values(streams_of[15], (D, CW), D ** -0.5, 0.125, ((0, 4), (1, 2)))
    pointwise_gate_weight = normal_values(streams_of[16], (D, CW), D ** -0.5, 0.125, ((0, 4), (1, 2)))
    depthwise_taps_weight = draw_depthwise_taps_weight(jax.random.fold_in(streams_of[21], 71), 0)
    channel_norm_scale = jnp.clip(1.0 + 0.18 * jax.random.normal(streams_of[18], (CW,), jnp.float32), 0.1, 1.9)
    mixer_output_weight = normal_values(streams_of[19], (RW_W, D), (RW_W + CW) ** -0.5, 0.15625, ((0, 2), (1, 4)))
    convolution_output_weight = normal_values(streams_of[20], (CW, D), (RW_W + CW) ** -0.5, 0.15625, ((0, 2), (1, 4)))
    return dict(inputs=inputs, input_norm_scale=input_norm_scale, query_matrix=query_matrix, key_matrix=key_matrix, value_matrix=value_matrix, decay_down_weight=decay_down_weight, decay_up_weight=decay_up_weight, decay_bias_base=decay_bias_base, decay_position_offset=decay_position_offset, extra_log_decay=extra_log_decay, correction_down_weight=correction_down_weight, correction_up_weight=correction_up_weight, correction_rate_bias=correction_rate_bias, head_norm_scale=head_norm_scale, starting_states=starting_states, pointwise_value_weight=pointwise_value_weight, pointwise_gate_weight=pointwise_gate_weight, depthwise_taps_weight=depthwise_taps_weight, channel_norm_scale=channel_norm_scale, mixer_output_weight=mixer_output_weight, convolution_output_weight=convolution_output_weight)


highest = lax.Precision.HIGHEST

def split_heads(values):
    return values.reshape(values.shape[0], -1, ATTN_GROUP_SIZE)

def paired(values):
    return jnp.stack([values, jnp.flip(values, 0)], 1)

def state_step(state, inputs):
    fading_multiplier, unit_key, rated_key, keys, values, query = inputs
    projected = jnp.einsum('dhvk,dhk->dhv', state, unit_key, precision=highest)
    state = state * fading_multiplier[:, :, None, :] - projected[..., None] * rated_key[:, :, None, :] + values[..., None] * keys[:, :, None, :]
    return (state, jnp.einsum('dhvk,dhk->dhv', state, query, precision=highest))

def head_norm(summed, head_norm_scale):
    centered = summed - lax.optimization_barrier(jnp.mean(summed, axis=-1, keepdims=True))
    scaled = centered * lax.rsqrt(lax.optimization_barrier(jnp.mean(centered * centered, axis=-1, keepdims=True)) + 0.00064)
    return (scaled * head_norm_scale.reshape(-1, ATTN_GROUP_SIZE)).reshape(summed.shape[0], -1).astype(jnp.bfloat16)

def reference(inputs, input_norm_scale, query_matrix, key_matrix, value_matrix, decay_down_weight, decay_up_weight, decay_bias_base, decay_position_offset, extra_log_decay, correction_down_weight, correction_up_weight, correction_rate_bias, head_norm_scale, starting_states, pointwise_value_weight, pointwise_gate_weight, depthwise_taps_weight, channel_norm_scale, mixer_output_weight, convolution_output_weight):

    def single_sequence(entry_collection):
        symbol_vectors, location_shift, fading_spike_amount, initial_memory_matrix = entry_collection
        as_float = symbol_vectors.astype(jnp.float32)
        normed = (as_float * lax.rsqrt(lax.optimization_barrier(jnp.mean(as_float * as_float, axis=-1, keepdims=True)) + 1e-06) * input_norm_scale).astype(jnp.bfloat16)

        def project(weight):
            return jnp.dot(normed, weight, preferred_element_type=jnp.float32)

        def rounded(total):
            return lax.optimization_barrier(total.astype(jnp.bfloat16)).astype(jnp.float32)
        query = rounded(project(query_matrix))
        keys = rounded(project(key_matrix))
        values = rounded(project(value_matrix))
        low_decay = jnp.tanh(project(decay_down_weight)).astype(jnp.bfloat16)
        fading_raw_scores = decay_bias_base + jnp.dot(low_decay, decay_up_weight, preferred_element_type=jnp.float32) + jnp.repeat(location_shift, ATTN_GROUP_SIZE, axis=1)
        fading_multiplier = jnp.exp(-jnp.exp(-jax.nn.softplus(-fading_raw_scores) - 0.5) + jnp.repeat(fading_spike_amount, ATTN_GROUP_SIZE, axis=1))
        low_rate = project(correction_down_weight).astype(jnp.bfloat16)
        rate = jax.nn.sigmoid(correction_rate_bias + jnp.dot(low_rate, correction_up_weight, preferred_element_type=jnp.float32))
        key_heads = split_heads(keys)
        unit_key = key_heads * lax.rsqrt(lax.optimization_barrier(jnp.sum(key_heads * key_heads, axis=-1, keepdims=True)) + 1e-06)
        rated_key = unit_key * split_heads(rate)
        steps = tuple((paired(item) for item in (split_heads(fading_multiplier), unit_key, rated_key, key_heads, split_heads(values), split_heads(query))))
        final, outputs = lax.scan(state_step, initial_memory_matrix, steps)
        summed = outputs[:, 0] + jnp.flip(outputs[:, 1], 0)
        mixer_out = head_norm(summed, head_norm_scale)
        glu = (project(pointwise_value_weight) * jax.nn.sigmoid(project(pointwise_gate_weight))).astype(jnp.bfloat16)
        reach = depthwise_taps_weight.shape[0] // 2
        padded = jnp.pad(glu.astype(jnp.float32), ((reach, reach), (0, 0)))
        conv = lax.conv_general_dilated(padded[None], depthwise_taps_weight[:, None, :], (1,), 'VALID', dimension_numbers=('NWC', 'WIO', 'NWC'), feature_group_count=depthwise_taps_weight.shape[1], precision=highest)[0]
        width = conv.shape[1]
        mean = lax.optimization_barrier(jnp.sum(conv, axis=-1)) / width
        power = lax.optimization_barrier(jnp.sum(conv * conv, axis=-1)) / width - mean * mean
        conv_out = jax.nn.silu((conv - mean[:, None]) * lax.rsqrt(power[:, None] + 1e-05) * channel_norm_scale).astype(jnp.bfloat16)
        total = jnp.dot(mixer_out, mixer_output_weight, preferred_element_type=jnp.float32) + jnp.dot(conv_out, convolution_output_weight, preferred_element_type=jnp.float32)
        return total.astype(jnp.bfloat16)
    return lax.map(single_sequence, (inputs, decay_position_offset, extra_log_decay, starting_states))
```

```python
import functools

import jax
import jax.numpy as jnp
from jax import lax
from jax.experimental import pallas as pl
from jax.experimental.pallas import tpu as pltpu
from jax.sharding import PartitionSpec as P

GROUP = 64
CHUNK = 64
MESH = pl.DeviceIdType.MESH
f32 = jnp.float32
bf16 = jnp.bfloat16
NN = (((1,), (0,)), ((), ()))
NT = (((1,), (1,)), ((), ()))
TN = (((0,), (0,)), ((), ()))


def dot1(a, b, dims=NN):
    return lax.dot_general(a, b, dims, preferred_element_type=f32)


def halves(a):
    hi = a.astype(bf16)
    return hi, (a - hi.astype(f32)).astype(bf16)


def dot3(a, b, dims=NN):
    a, b = (x if isinstance(x, tuple) else halves(x) for x in (a, b))
    return dot1(a[0], b[0], dims) + (dot1(a[0], b[1], dims) + dot1(a[1], b[0], dims))


def exact_left(mask, x):
    hi, rest = x.astype(bf16), x - x.astype(bf16).astype(f32)
    mid, low = halves(rest)
    return dot1(mask, hi) + (dot1(mask, mid) + dot1(mask, low))


def remote(src, dst, send, recv, where):
    return pltpu.make_async_remote_copy(
        src_ref=src, dst_ref=dst, send_sem=send, recv_sem=recv, device_id=where, device_id_type=MESH
    )


def greet(peers):
    barrier = pltpu.get_barrier_semaphore()
    for where in peers:
        pl.semaphore_signal(barrier, inc=1, device_id=where, device_id_type=MESH)
    pl.semaphore_wait(barrier, len(peers))


def collect_kernel(n, m, x_ref, w_ref, e_ref, xo, wo, eo, local, xsend, xrecv, dsend, drecv, wsend, wrecv, esend, erecv):
    s, t = lax.axis_index("sp"), lax.axis_index("tp")
    rows, feats = x_ref.shape
    depth = w_ref.shape[1]

    def slot(b, c):
        return xo.at[pl.ds(b * rows, rows), pl.ds(pl.multiple_of(c * feats, feats), feats)]

    own_x = pltpu.make_async_copy(x_ref, slot(s, t), local.at[0])
    own_w = pltpu.make_async_copy(w_ref.at[s], wo.at[pl.ds(s * depth, depth)], local.at[1])
    own_e = pltpu.make_async_copy(e_ref, eo.at[s], local.at[2])
    for copy in (own_x, own_w, own_e):
        copy.start()
    ring = [lax.rem(s + k, n) for k in range(1, n)]
    mates = [lax.rem(t + k, m) for k in range(1, m)]
    greet([{"sp": p} for p in ring] + [{"tp": c} for c in mates])

    def along(k, way):
        b = s - k if way == 0 else s + k
        src = x_ref if k == 0 else slot(b, t)
        return remote(src, slot(b, t), xsend.at[way, k], xrecv.at[way, k], {"sp": s + 1 if way == 0 else s - 1})

    def sends(k, way):
        return (s - k >= 0) & (s < n - 1) if way == 0 else (s + k < n) & (s > 0)

    def gets(k, way):
        return s - 1 - k >= 0 if way == 0 else s + 1 + k < n

    def across(index, j, b):
        src = x_ref if index == 0 else slot(b, t)
        return remote(src, slot(b, t), dsend.at[index, j], drecv.at[index, j], {"tp": mates[j]})

    def across_in(index, j, b):
        c = lax.rem(t + m - 1 - j, m)
        return remote(slot(b, c), slot(b, c), dsend.at[index, j], drecv.at[index, j], {"tp": mates[j]})

    for way in range(2):
        @pl.when(sends(0, way))
        def _():
            along(0, way).start()
    extras = []
    for k in range(1, n):
        copy = remote(e_ref, eo.at[s], esend.at[k - 1], erecv.at[k - 1], {"sp": ring[k - 1]})
        copy.start()
        extras.append(copy)
    weights = []
    for k in range(1, n):
        p = ring[k - 1]
        copy = remote(
            w_ref.at[p], wo.at[pl.ds(s * depth, depth)], wsend.at[k - 1], wrecv.at[k - 1], {"sp": p}
        )
        copy.start()
        weights.append(copy)
    for j in range(m - 1):
        across(0, j, s).start()
    for k in range(n - 1):
        for way in range(2):
            @pl.when(gets(k, way))
            def _():
                b = s - 1 - k if way == 0 else s + 1 + k
                remote(slot(b, t), slot(b, t), xsend.at[way, k], xrecv.at[way, k], {"sp": b}).wait_recv()
                if k + 1 < n - 1:
                    @pl.when(sends(k + 1, way))
                    def _():
                        along(k + 1, way).start()
                for j in range(m - 1):
                    across(1 + 2 * k + way, j, b).start()
    for j in range(m - 1):
        across_in(0, j, s).wait_recv()
        across(0, j, s).wait_send()
    for k in range(n - 1):
        for way in range(2):
            @pl.when(gets(k, way))
            def _():
                b = s - 1 - k if way == 0 else s + 1 + k
                for j in range(m - 1):
                    across_in(1 + 2 * k + way, j, b).wait_recv()
                    across(1 + 2 * k + way, j, b).wait_send()

            @pl.when(sends(k, way))
            def _():
                along(k, way).wait_send()
    for k in range(1, n):
        p = lax.rem(s + n - k, n)
        remote(eo.at[p], eo.at[p], esend.at[k - 1], erecv.at[k - 1], {"sp": p}).wait_recv()
        part = wo.at[pl.ds(p * depth, depth)]
        remote(part, part, wsend.at[k - 1], wrecv.at[k - 1], {"sp": p}).wait_recv()
        extras[k - 1].wait_send()
        weights[k - 1].wait_send()
    for copy in (own_x, own_w, own_e):
        copy.wait()


def collect(n, m, x, w, e):
    rows, feats = x.shape
    vmem = pl.BlockSpec(memory_space=pltpu.VMEM)
    dma = pltpu.SemaphoreType.DMA
    hops = max(n - 1, 1)
    return pl.pallas_call(
        functools.partial(collect_kernel, n, m),
        out_shape=(
            jax.ShapeDtypeStruct((n * rows, m * feats), bf16),
            jax.ShapeDtypeStruct((n * w.shape[1], w.shape[2]), bf16),
            jax.ShapeDtypeStruct((n,) + e.shape, f32),
        ),
        in_specs=[vmem] * 3,
        out_specs=(vmem,) * 3,
        scratch_shapes=[
            dma((3,)),
            dma((2, hops)), dma((2, hops)),
            dma((2 * n - 1, max(m - 1, 1))), dma((2 * n - 1, max(m - 1, 1))),
            dma((hops,)), dma((hops,)), dma((hops,)), dma((hops,)),
        ],
        compiler_params=pltpu.CompilerParams(collective_id=0, has_side_effects=True),
    )(x, w, e)


def pick(ref, s, n, width):
    out = ref[:, :width]
    for i in range(1, n):
        out = jnp.where(s == i, ref[:, i * width : (i + 1) * width], out)
    return out


def mix_kernel(
    n, m, hc, cc, rows,
    x_ref, gain_ref, w_ref, e_ref, dd_ref, du_ref, db_ref, cd_ref, cu_ref, cb_ref, hs_ref, st_ref, taps_ref,
    mix_ref, conv_ref, sums_ref,
    proj, low, glu, maps, adds, qe, oi, states,
):
    s = lax.axis_index("sp")
    heads = hc // GROUP
    length = x_ref.shape[0]
    feats = x_ref.shape[1]
    block = 256 if length % 256 == 0 else rows

    @pl.loop(0, length // block)
    def _(i):
        at = pl.ds(pl.multiple_of(i * block, block), block)
        x = x_ref[at, :].astype(f32)
        normed = (x * lax.rsqrt(jnp.mean(x * x, axis=-1, keepdims=True) + 1e-06) * gain_ref[...]).astype(bf16)
        proj[at, :] = dot1(normed, w_ref[...])
        low[0, at, :] = jnp.tanh(dot1(normed, dd_ref[...])).astype(bf16)
        low[1, at, :] = dot1(normed, cd_ref[...]).astype(bf16)

    reach = taps_ref.shape[0] // 2
    top = 16 * ((reach + 15) // 16)
    glu[pl.ds(0, top), :] = jnp.zeros((top, cc), f32)
    glu[pl.ds(top + length, top), :] = jnp.zeros((top, cc), f32)
    base = 2 * hc
    gate = proj[:, base + cc : base + 2 * cc]
    glu[pl.ds(top, length), :] = (proj[:, base : base + cc] * jax.nn.sigmoid(gate)).astype(bf16).astype(f32)
    taps = pick(taps_ref, s, n, cc)
    step = 64
    for r in range(0, length, step):
        total = jnp.zeros((step, cc), f32)
        for j in range(taps_ref.shape[0]):
            total += taps[j : j + 1, :] * glu[pl.ds(r + top - reach + j, step), :]
        conv_ref[pl.ds(r, step), :] = total
    ones = jnp.ones((8, cc), f32)
    conv = conv_ref[...]
    row = lax.broadcasted_iota(jnp.int32, (8, length), 0)
    first = exact_rows(ones, conv)
    second = exact_rows(ones, conv * conv)
    sums_ref[...] = jnp.where(row == 0, first, jnp.where(row == 1, second, 0.0))

    size = 2 * CHUNK if rows % (2 * CHUNK) == 0 else CHUNK
    per = size // CHUNK
    ti = lax.broadcasted_iota(jnp.int32, (size, size), 0)
    tj = lax.broadcasted_iota(jnp.int32, (size, size), 1)
    same = ti // CHUNK == tj // CHUNK
    whole = same.astype(f32).astype(bf16)
    eye = (ti == tj).astype(f32)
    small_eye = (
        lax.broadcasted_iota(jnp.int32, (GROUP, GROUP), 0) == lax.broadcasted_iota(jnp.int32, (GROUP, GROUP), 1)
    ).astype(f32)
    du, cu = pick(du_ref, s, n, hc), pick(cu_ref, s, n, hc)
    db, cb = pick(db_ref, s, n, hc), pick(cb_ref, s, n, hc)
    hs = pick(hs_ref, s, n, hc)
    local_heads = e_ref.shape[1] // 2
    erow = lax.broadcasted_iota(jnp.int32, (2 * local_heads, GROUP), 0)

    for h in range(heads):
        lanes = slice(h * GROUP, (h + 1) * GROUP)
        klanes = slice(hc + h * GROUP, hc + (h + 1) * GROUP)
        vlanes = slice(base + 2 * cc + h * GROUP, base + 2 * cc + (h + 1) * GROUP)
        pick_offset = (erow == s * heads + h).astype(f32)
        pick_extra = (erow == local_heads + s * heads + h).astype(f32)

        @pl.loop(0, length // size)
        def _(i):
            at = pl.ds(pl.multiple_of(i * size, size), size)
            inner = rows // size
            if inner == 1:
                entry = e_ref[i]
            else:
                entry = e_ref[i // inner, :, pl.ds(pl.multiple_of((i % inner) * size, size), size)]
            offset = lax.dot_general(entry, pick_offset, TN, precision=lax.Precision.HIGHEST, preferred_element_type=f32)
            extra = lax.dot_general(entry, pick_extra, TN, precision=lax.Precision.HIGHEST, preferred_element_type=f32)
            pre = db[:, lanes] + dot1(low[0, at, :], du[:, lanes]) + offset
            lw = -jnp.exp(-jax.nn.softplus(-pre) - 0.5) + extra
            rate = jax.nn.sigmoid(cb[:, lanes] + dot1(low[1, at, :], cu[:, lanes]))
            q = proj[at, lanes].astype(bf16).astype(f32)
            k = proj[at, klanes].astype(bf16).astype(f32)
            vb = proj[at, vlanes].astype(bf16)
            unit = k * lax.rsqrt(jnp.sum(k * k, axis=-1, keepdims=True) + 1e-06)
            rated = unit * rate
            total = exact_left(whole, lw)
            for d in range(2):
                strict = same & ((ti > tj) if d == 0 else (ti < tj))
                upto = same & ((ti >= tj) if d == 0 else (ti <= tj))
                g = exact_left(upto.astype(f32).astype(bf16), lw)
                before = g - lw
                middle = 0.5 * total
                ahead = jnp.exp(middle - g)
                left = halves(jnp.concatenate([unit * jnp.exp(before - middle), q * jnp.exp(g - middle)], axis=0))
                right = halves(jnp.concatenate([rated * ahead, k * ahead], axis=0))
                scores = dot3(left, right, NT)
                a_ur = jnp.where(strict, scores[:size, :size], 0.0)
                a_uk = jnp.where(strict, scores[:size, size:], 0.0)
                a_qr = jnp.where(upto, scores[size:, :size], 0.0)
                a_qk = jnp.where(upto, scores[size:, size:], 0.0)
                width = 1
                inverse = eye - jnp.where((ti // 2 == tj // 2), a_ur, 0.0)
                width = 2
                while width < CHUNK:
                    part = jnp.where(
                        (ti // (2 * width) == tj // (2 * width)) & (ti // width != tj // width), a_ur, 0.0
                    )
                    pair = halves(inverse)
                    inverse = inverse - dot3(dot3(pair, part), pair)
                    width *= 2
                a_kv = halves(jnp.concatenate([a_uk, a_qk], axis=0))
                both = dot1(a_kv[0], vb) + dot1(a_kv[1], vb)
                wy = dot3(inverse, jnp.concatenate([unit * jnp.exp(before), both[:size]], axis=1))
                far = dot3(a_qr, wy)
                qe[d, at, :] = q * jnp.exp(g) - far[:, :GROUP]
                oi[d, at, :] = both[size:] - far[:, GROUP:]
                tail = jnp.exp(total - g)
                r_end, k_end = rated * tail, k * tail
                for c in range(per):
                    cut = slice(c * CHUNK, (c + 1) * CHUNK)
                    moved = dot3(wy[cut], r_end[cut], TN)
                    ke = halves(k_end[cut])
                    came = dot1(vb[cut], ke[0], TN) + dot1(vb[cut], ke[1], TN)
                    decay = jnp.exp(total[c * CHUNK : c * CHUNK + 1])
                    maps[d, i * per + c] = small_eye * decay - moved[:GROUP]
                    adds[d, i * per + c] = came - moved[GROUP:]

        chunks = length // CHUNK
        now = [st_ref[0, 0, s * heads + h], st_ref[0, 1, s * heads + h]]
        for c in range(chunks):
            for d in range(2):
                at = c if d == 0 else chunks - 1 - c
                states[d, at] = now[d]
                if c < chunks - 1:
                    now[d] = dot3(now[d], maps[d, at]) + adds[d, at]
        share = rows // m
        for c in range(chunks):
            cut = pl.ds(c * CHUNK, CHUNK)
            out = oi[0, cut, :] + oi[1, cut, :]
            for d in range(2):
                out += dot3(qe[d, cut, :], states[d, c], NT)
            centered = out - jnp.mean(out, axis=-1, keepdims=True)
            power = jnp.mean(centered * centered, axis=-1, keepdims=True)
            done = (centered * lax.rsqrt(power + 0.00064) * hs[:, lanes]).astype(bf16)
            for piece in range(0, CHUNK, min(share, CHUNK)):
                token = c * CHUNK + piece
                take = min(share, CHUNK)
                owner, inside = token // rows, token % rows
                mix_ref[inside // share, pl.ds(owner * share + inside % share, take), lanes] = done[piece : piece + take]


def exact_rows(ones, x):
    return lax.dot_general(ones, x, NT, precision=lax.Precision.HIGHEST, preferred_element_type=f32)


def mix(n, m, hc, cc, rows, *args):
    length = args[0].shape[0]
    vmem = pl.BlockSpec(memory_space=pltpu.VMEM)
    rank = args[4].shape[1]
    reach = args[12].shape[0] // 2
    top = 16 * ((reach + 15) // 16)
    chunks = length // CHUNK
    return pl.pallas_call(
        functools.partial(mix_kernel, n, m, hc, cc, rows),
        out_shape=(
            jax.ShapeDtypeStruct((m, length // m, hc), bf16),
            jax.ShapeDtypeStruct((length, cc), f32),
            jax.ShapeDtypeStruct((8, length), f32),
        ),
        in_specs=[vmem] * len(args),
        out_specs=(vmem,) * 3,
        scratch_shapes=[
            pltpu.VMEM((length, args[2].shape[1]), f32),
            pltpu.VMEM((2, length, rank), bf16),
            pltpu.VMEM((length + 2 * top, cc), f32),
            pltpu.VMEM((2, chunks, GROUP, GROUP), f32),
            pltpu.VMEM((2, chunks, GROUP, GROUP), f32),
            pltpu.VMEM((2, length, GROUP), f32),
            pltpu.VMEM((2, length, GROUP), f32),
            pltpu.VMEM((2, chunks, GROUP, GROUP), f32),
        ],
    )(*args)


def output_kernel(
    n, m, hc, cc, pack,
    mix_ref, conv_ref, sums_ref, cs_ref, wm_ref, wc_ref, out_ref,
    own, around, mates_act, sums_in, wm_in, wc_in, total, block,
    local, ssend, srecv, vsend, vrecv, asend, arecv, dsend, drecv, osend, orecv,
):
    s, t = lax.axis_index("sp"), lax.axis_index("tp")
    here = s * m + t
    everyone = n * m
    length = conv_ref.shape[0]
    half = length // m
    share = half // n
    columns = wm_ref.shape[1]
    packed = half // pack
    mates = [lax.rem(t + k, m) for k in range(1, m)]

    def other(k):
        p = lax.rem(here + k, everyone)
        return {"sp": p // m, "tp": p % m}

    greet([other(k) for k in range(1, everyone)])
    outs = []
    for k in range(1, everyone):
        outs.append(remote(sums_ref, sums_in.at[k - 1], ssend.at[k - 1], srecv.at[k - 1], other(k)))
    for j in range(m - 1):
        outs.append(remote(wm_ref, wm_in.at[j], vsend.at[0, j], vrecv.at[0, j], {"tp": mates[j]}))
        outs.append(remote(wc_ref, wc_in.at[j], vsend.at[1, j], vrecv.at[1, j], {"tp": mates[j]}))
    for copy in outs:
        copy.start()
    width = mix_ref.shape[2]
    for c in range(m):
        for i in range(pack):
            own[c, pl.ds(0, packed), pl.ds(i * hc, hc)] = mix_ref[c, pl.ds(i * packed, packed), :]
    for copy in outs[: everyone - 1]:
        copy.wait()
    stats = sums_ref[...]
    for k in range(everyone - 1):
        stats += sums_in[k]
    row = lax.broadcasted_iota(jnp.int32, (8, cc), 0)
    channels = cc * n * m

    def spread(which):
        return lax.dot_general(
            stats, (row == which).astype(f32), TN, precision=lax.Precision.HIGHEST, preferred_element_type=f32
        )

    mean = spread(0) / channels
    power = spread(1) / channels - mean * mean
    gain = pick(cs_ref, s, n, cc)
    done = jax.nn.silu((conv_ref[...] - mean) * lax.rsqrt(power + 1e-05) * gain).astype(bf16)
    for token in range(0, length, share):
        unit = token // share
        own[unit % m, pl.ds(packed + (unit // m) * share, share), :] = done[token : token + share]

    def along(k, way):
        b = s - k if way == 0 else s + k
        src = own if k == 0 else around.at[b]
        return remote(src, around.at[b], asend.at[way, k], arecv.at[way, k], {"sp": s + 1 if way == 0 else s - 1})

    def sends(k, way):
        return (s - k >= 0) & (s < n - 1) if way == 0 else (s + k < n) & (s > 0)

    def gets(k, way):
        return s - 1 - k >= 0 if way == 0 else s + 1 + k < n

    def across(index, j, b):
        src = own.at[mates[j]] if index == 0 else around.at[b, mates[j]]
        return remote(src, mates_act.at[j, b], dsend.at[index, j], drecv.at[index, j], {"tp": mates[j]})

    def add(b, act, wm, wc):
        w = wm[pl.ds(pl.multiple_of(b * hc, hc), hc), :]
        for i in range(pack):
            rows = pl.ds(i * packed, packed)
            total[rows, :] += dot1(act[pl.ds(0, packed), pl.ds(i * hc, hc)], w)
        total[...] += dot1(act[pl.ds(packed, half), :], wc[pl.ds(pl.multiple_of(b * cc, cc), cc), :])

    for way in range(2):
        @pl.when(sends(0, way))
        def _():
            along(0, way).start()
    for j in range(m - 1):
        across(0, j, s).start()
    total[...] = jnp.zeros_like(total)
    add(s, own.at[t], wm_ref, wc_ref)
    for copy in outs[everyone - 1 :]:
        copy.wait()

    def from_mates(index, b):
        for j in range(m - 1):
            across(index, j, b).wait_recv()
            add(b, mates_act.at[j, b], wm_in.at[j], wc_in.at[j])
            across(index, j, b).wait_send()

    for k in range(n - 1):
        for way in range(2):
            @pl.when(gets(k, way))
            def _():
                b = s - 1 - k if way == 0 else s + 1 + k
                remote(around.at[b], around.at[b], asend.at[way, k], arecv.at[way, k], {"sp": b}).wait_recv()
                if k + 1 < n - 1:
                    @pl.when(sends(k + 1, way))
                    def _():
                        along(k + 1, way).start()
                for j in range(m - 1):
                    across(1 + 2 * k + way, j, b).start()
                add(b, around.at[b, t], wm_ref, wc_ref)
        if k == 0:
            from_mates(0, s)
        else:
            for way in range(2):
                @pl.when(gets(k - 1, way))
                def _():
                    from_mates(2 * k - 1 + way, s - k if way == 0 else s + k)
    for way in range(2):
        @pl.when(gets(n - 2, way))
        def _():
            from_mates(2 * n - 3 + way, s - n + 1 if way == 0 else s + n - 1)
    for k in range(n - 1):
        for way in range(2):
            @pl.when(sends(k, way))
            def _():
                along(k, way).wait_send()
    block[...] = total[...].astype(bf16)
    mine = out_ref.at[:, pl.ds(pl.multiple_of(s * columns, columns), columns)]
    keep = pltpu.make_async_copy(block.at[pl.ds(s * share, share)], mine, local.at[0])
    keep.start()
    final = []
    for k in range(1, n):
        p = lax.rem(s + k, n)
        copy = remote(block.at[pl.ds(p * share, share)], mine, osend.at[k - 1], orecv.at[k - 1], {"sp": p})
        copy.start()
        final.append(copy)
    for k in range(1, n):
        p = lax.rem(s + n - k, n)
        part = out_ref.at[:, pl.ds(pl.multiple_of(p * columns, columns), columns)]
        remote(part, part, osend.at[k - 1], orecv.at[k - 1], {"sp": p}).wait_recv()
        final[k - 1].wait_send()
    keep.wait()


def output(n, m, hc, cc, mixed, conv, sums, cs, wm, wc):
    length = conv.shape[0]
    half, columns = length // m, wm.shape[1]
    pack = max(cc // hc, 1)
    rows = half // pack + half
    vmem = pl.BlockSpec(memory_space=pltpu.VMEM)
    dma = pltpu.SemaphoreType.DMA
    hops, mates = max(n - 1, 1), max(m - 1, 1)
    return pl.pallas_call(
        functools.partial(output_kernel, n, m, hc, cc, pack),
        out_shape=jax.ShapeDtypeStruct((half // n, n * columns), bf16),
        in_specs=[vmem] * 6,
        out_specs=vmem,
        scratch_shapes=[
            pltpu.VMEM((m, rows, cc), bf16),
            pltpu.VMEM((n, m, rows, cc), bf16),
            pltpu.VMEM((mates, n, rows, cc), bf16),
            pltpu.VMEM((n * m - 1, 8, length), f32),
            pltpu.VMEM((mates,) + wm.shape, bf16),
            pltpu.VMEM((mates,) + wc.shape, bf16),
            pltpu.VMEM((half, columns), f32),
            pltpu.VMEM((half, columns), bf16),
            dma((1,)),
            dma((n * m - 1,)), dma((n * m - 1,)),
            dma((2, mates)), dma((2, mates)),
            dma((2, hops)), dma((2, hops)),
            dma((2 * n - 1, mates)), dma((2 * n - 1, mates)),
            dma((hops,)), dma((hops,)),
        ],
        compiler_params=pltpu.CompilerParams(collective_id=1, has_side_effects=True),
    )(mixed, conv, sums, cs, wm, wc)


highest = lax.Precision.HIGHEST


def carried_in(x, axis, combine, identity, reverse):
    length, here = (lax.axis_size(axis), lax.axis_index(axis))
    everything = jax.tree.map(
        lambda part, kind: lax.all_gather(part.astype(kind), axis), x, (jnp.bfloat16, jnp.bfloat16)
    )
    start = jax.tree.map(
        lambda part, zero: jnp.broadcast_to(jnp.asarray(zero, part.dtype), part.shape), x, identity
    )

    def hop(k, before):
        at = length - 1 - k if reverse else k
        reached = at > here if reverse else at < here
        new = combine(
            before, jax.tree.map(lambda part, own: part[at].astype(own.dtype), everything, x)
        )
        return jax.tree.map(lambda a, b: jnp.where(reached, a, b), new, before)

    return lax.fori_loop(0, length, hop, start)


def padded_2(block, sides, width):
    for axis, dim in sides:
        count = lax.axis_size(axis)
        forward = [(i, i + 1) for i in range(count - 1)]
        backward = [(target, source) for source, target in forward]
        low = lax.ppermute(
            lax.slice_in_dim(block, block.shape[dim] - width, None, axis=dim), axis, forward
        )
        high = lax.ppermute(lax.slice_in_dim(block, 0, width, axis=dim), axis, backward)
        block = jnp.concatenate([low, block, high], axis=dim)
    return block


def split_heads(values):
    return values.reshape(values.shape[0], -1, GROUP)


def paired(values):
    return jnp.stack([values, jnp.flip(values, 0)], 1)


def local_step(stacked, inputs):
    fading_multiplier, unit_key, rated_key, keys, values, query = inputs
    projected = jnp.einsum("dhvk,dhk->dhv", stacked, unit_key, precision=highest)
    outer = values[..., None] * keys[:, :, None, :]
    added = jnp.concatenate([jnp.zeros_like(outer), outer], axis=2)
    stacked = (
        stacked * fading_multiplier[:, :, None, :]
        - projected[..., None] * rated_key[:, :, None, :]
        + added
    )
    return (stacked, jnp.einsum("dhvk,dhk->dhv", stacked, query, precision=highest))


def chain_pair(earlier, later):
    product = jnp.einsum("hij,hjk->hik", earlier[0], later[0], precision=highest)
    moved = jnp.einsum("hij,hjk->hik", earlier[1], later[0], precision=highest) + later[1]
    return (product, moved)


def carry_in(initial_memory_matrix, prefix):
    return (
        jnp.einsum("hij,hjk->hik", initial_memory_matrix, prefix[0], precision=highest) + prefix[1]
    )


def head_norm(summed, head_norm_scale):
    centered = summed - jnp.mean(summed, axis=-1, keepdims=True)
    scaled = centered * lax.rsqrt(jnp.mean(centered * centered, axis=-1, keepdims=True) + 0.00064)
    return (
        (scaled * head_norm_scale.reshape(-1, GROUP))
        .reshape(summed.shape[0], -1)
        .astype(jnp.bfloat16)
    )


def rounded(total):
    return lax.optimization_barrier(total.astype(jnp.bfloat16)).astype(jnp.float32)


def mixer_branch(
    normed,
    sums,
    decay_down_weight,
    decay_up_weight,
    decay_bias_base,
    decay_position_offset,
    extra_log_decay,
    correction_down_weight,
    correction_up_weight,
    correction_rate_bias,
    head_norm_scale,
    starting_states,
):
    query = rounded(sums[0])
    keys = rounded(sums[1])
    values = rounded(sums[2])
    low_decay = jnp.tanh(
        jnp.dot(normed, decay_down_weight, preferred_element_type=jnp.float32)
    ).astype(jnp.bfloat16)
    fading_raw_scores = (
        decay_bias_base
        + jnp.dot(low_decay, decay_up_weight, preferred_element_type=jnp.float32)
        + jnp.repeat(decay_position_offset[0], GROUP, axis=1)
    )
    fading_multiplier = jnp.exp(
        -jnp.exp(-jax.nn.softplus(-fading_raw_scores) - 0.5)
        + jnp.repeat(extra_log_decay[0], GROUP, axis=1)
    )
    low_rate = jnp.dot(normed, correction_down_weight, preferred_element_type=jnp.float32).astype(
        jnp.bfloat16
    )
    rate = jax.nn.sigmoid(
        correction_rate_bias
        + jnp.dot(low_rate, correction_up_weight, preferred_element_type=jnp.float32)
    )
    key_heads = split_heads(keys)
    unit_key = key_heads * lax.rsqrt(jnp.sum(key_heads * key_heads, axis=-1, keepdims=True) + 1e-06)
    rated_key = unit_key * split_heads(rate)
    steps = tuple(
        (
            paired(item)
            for item in (
                split_heads(fading_multiplier),
                unit_key,
                rated_key,
                key_heads,
                split_heads(values),
                split_heads(query),
            )
        )
    )
    heads_here = key_heads.shape[1]
    identity = jnp.broadcast_to(
        jnp.eye(GROUP, dtype=jnp.float32),
        (2, heads_here, GROUP, GROUP),
    )
    nothing = jnp.zeros((2, heads_here, GROUP, GROUP), jnp.float32)
    start = jnp.concatenate([identity, nothing], axis=2)
    ends, emitted = lax.scan(local_step, start, steps, unroll=8)
    transfer = ends[:, :, :GROUP]
    alone = ends[:, :, GROUP:]
    through = emitted[..., :GROUP]
    own_part = emitted[..., GROUP:]
    before = carried_in((transfer[0], alone[0]), "sp", chain_pair, (identity[0], nothing[0]), False)
    after = carried_in((transfer[1], alone[1]), "sp", chain_pair, (identity[1], nothing[1]), True)
    starts = jnp.stack(
        [carry_in(starting_states[0, 0], before), carry_in(starting_states[0, 1], after)], 0
    )
    outputs = jnp.einsum("dhvk,tdhk->tdhv", starts, through, precision=highest) + own_part
    summed = outputs[:, 0] + jnp.flip(outputs[:, 1], 0)
    return head_norm(summed, head_norm_scale)


def conv_branch(sums, depthwise_taps_weight, channel_norm_scale):
    glu = (sums[0] * jax.nn.sigmoid(sums[1])).astype(jnp.bfloat16)
    reach = depthwise_taps_weight.shape[0] // 2
    padded = padded_2(glu, (("sp", 0),), reach)
    conv = lax.conv_general_dilated(
        padded.astype(jnp.float32)[None],
        depthwise_taps_weight[:, None, :],
        (1,),
        "VALID",
        dimension_numbers=("NWC", "WIO", "NWC"),
        feature_group_count=depthwise_taps_weight.shape[1],
        precision=highest,
    )[0]
    first, second = lax.psum((jnp.sum(conv, axis=-1), jnp.sum(conv * conv, axis=-1)), "tp")
    width = conv.shape[1] * lax.axis_size("tp")
    mean = first / width
    power = second / width - mean * mean
    return jax.nn.silu(
        (conv - mean[:, None]) * lax.rsqrt(power[:, None] + 1e-05) * channel_norm_scale
    ).astype(jnp.bfloat16)


def spread_device(
    inputs,
    input_norm_scale,
    query_matrix,
    key_matrix,
    value_matrix,
    decay_down_weight,
    decay_up_weight,
    decay_bias_base,
    decay_position_offset,
    extra_log_decay,
    correction_down_weight,
    correction_up_weight,
    correction_rate_bias,
    head_norm_scale,
    starting_states,
    pointwise_value_weight,
    pointwise_gate_weight,
    depthwise_taps_weight,
    channel_norm_scale,
    mixer_output_weight,
    convolution_output_weight,
):
    symbol_vectors = lax.all_gather(inputs[0], "tp", axis=1, tiled=True)
    as_float = symbol_vectors.astype(jnp.float32)
    normed = (
        as_float
        * lax.rsqrt(jnp.mean(as_float * as_float, axis=-1, keepdims=True) + 1e-06)
        * input_norm_scale
    ).astype(jnp.bfloat16)
    mixer_args = (
        decay_down_weight,
        decay_up_weight,
        decay_bias_base,
        decay_position_offset,
        extra_log_decay,
        correction_down_weight,
        correction_up_weight,
        correction_rate_bias,
        head_norm_scale,
        starting_states,
    )
    pieces = (
        lax.all_gather(query_matrix, "sp", axis=0, tiled=True),
        lax.all_gather(key_matrix, "sp", axis=0, tiled=True),
        lax.all_gather(value_matrix, "sp", axis=0, tiled=True),
        lax.all_gather(pointwise_value_weight, "sp", axis=0, tiled=True),
        lax.all_gather(pointwise_gate_weight, "sp", axis=0, tiled=True),
    )
    sums = tuple((jnp.dot(normed, piece, preferred_element_type=jnp.float32) for piece in pieces))
    mixer_out = mixer_branch(normed, sums[:3], *mixer_args)
    conv_out = conv_branch(sums[3:], depthwise_taps_weight, channel_norm_scale)
    joined = jnp.concatenate([mixer_out, conv_out], axis=1)
    weight_rows = jnp.concatenate([mixer_output_weight, convolution_output_weight], axis=0)
    columns = lax.all_gather(weight_rows, "sp", axis=1, tiled=True)
    moved = lax.all_to_all(joined, "tp", split_axis=0, concat_axis=1, tiled=True)
    every_row = lax.all_gather(columns, "tp", axis=0, tiled=True)
    total = jnp.dot(moved, every_row, preferred_element_type=jnp.float32)
    return total.astype(jnp.bfloat16)[None]


def per_device(
    inputs, input_norm_scale, query_matrix, key_matrix, value_matrix,
    decay_down_weight, decay_up_weight, decay_bias_base, decay_position_offset, extra_log_decay,
    correction_down_weight, correction_up_weight, correction_rate_bias, head_norm_scale, starting_states,
    pointwise_value_weight, pointwise_gate_weight, depthwise_taps_weight, channel_norm_scale,
    mixer_output_weight, convolution_output_weight,
):
    n, m = lax.axis_size("sp"), lax.axis_size("tp")
    if query_matrix.shape[1] % (n * GROUP) or pointwise_value_weight.shape[1] % (n * 128):
        return spread_device(
            inputs, input_norm_scale, query_matrix, key_matrix, value_matrix,
            decay_down_weight, decay_up_weight, decay_bias_base, decay_position_offset, extra_log_decay,
            correction_down_weight, correction_up_weight, correction_rate_bias, head_norm_scale, starting_states,
            pointwise_value_weight, pointwise_gate_weight, depthwise_taps_weight, channel_norm_scale,
            mixer_output_weight, convolution_output_weight,
        )
    x = inputs[0]
    rows = x.shape[0]
    depth = query_matrix.shape[0]
    hc, cc = query_matrix.shape[1] // n, pointwise_value_weight.shape[1] // n
    parts = [query_matrix, key_matrix, pointwise_value_weight, pointwise_gate_weight, value_matrix]
    w = jnp.concatenate([part.reshape(depth, n, -1) for part in parts], axis=2).transpose(1, 0, 2)
    e = jnp.concatenate([decay_position_offset[0], extra_log_decay[0]], axis=1).T
    everything, columns, shifts = collect(n, m, x, w, e)
    mixed, conv, sums = mix(
        n, m, hc, cc, rows,
        everything, input_norm_scale[None], columns, shifts,
        decay_down_weight, decay_up_weight, decay_bias_base[None],
        correction_down_weight, correction_up_weight, correction_rate_bias[None],
        head_norm_scale[None], starting_states, depthwise_taps_weight,
    )
    return output(
        n, m, hc, cc, mixed, conv, sums, channel_norm_scale[None], mixer_output_weight, convolution_output_weight
    )[None]


def solution(mesh):
    return jax.shard_map(
        per_device,
        mesh=mesh,
        in_specs=(
            P("fs", "sp", "tp"),
            P(),
            P("sp", "tp"),
            P("sp", "tp"),
            P("sp", "tp"),
            P(),
            P(None, "tp"),
            P("tp"),
            P("fs", "sp", "tp"),
            P("fs", "sp", "tp"),
            P(),
            P(None, "tp"),
            P("tp"),
            P("tp"),
            P("fs", None, "tp", None, None),
            P("sp", "tp"),
            P("sp", "tp"),
            P(None, "tp"),
            P("tp"),
            P("tp", "sp"),
            P("tp", "sp"),
        ),
        out_specs=P("fs", ("sp", "tp"), None),
        check_vma=False,
    )
```

```python
import functools

import jax
import jax.numpy as jnp
from jax import lax
from jax.experimental import pallas as pl
from jax.experimental.pallas import tpu as pltpu
from jax.sharding import PartitionSpec as P

GROUP = 64
CHUNK = 64
MESH = pl.DeviceIdType.MESH
f32 = jnp.float32
bf16 = jnp.bfloat16
NN = (((1,), (0,)), ((), ()))
NT = (((1,), (1,)), ((), ()))
TN = (((0,), (0,)), ((), ()))


def dot1(a, b, dims=NN):
    return lax.dot_general(a, b, dims, preferred_element_type=f32)


def halves(a):
    hi = a.astype(bf16)
    return hi, (a - hi.astype(f32)).astype(bf16)


def dot3(a, b, dims=NN):
    a, b = (x if isinstance(x, tuple) else halves(x) for x in (a, b))
    return dot1(a[0], b[0], dims) + (dot1(a[0], b[1], dims) + dot1(a[1], b[0], dims))


def exact_left(mask, x):
    hi, rest = x.astype(bf16), x - x.astype(bf16).astype(f32)
    mid, low = halves(rest)
    return dot1(mask, hi) + (dot1(mask, mid) + dot1(mask, low))


def remote(src, dst, send, recv, where):
    return pltpu.make_async_remote_copy(
        src_ref=src, dst_ref=dst, send_sem=send, recv_sem=recv, device_id=where, device_id_type=MESH
    )


def greet(peers):
    barrier = pltpu.get_barrier_semaphore()
    for where in peers:
        pl.semaphore_signal(barrier, inc=1, device_id=where, device_id_type=MESH)
    pl.semaphore_wait(barrier, len(peers))


def pick_lanes(ref, p, width):
    return ref[:, p * width : (p + 1) * width]


def collect_kernel(
    n, m, nf, cut,
    x_ref, q_ref, k_ref, pv_ref, pg_ref, v_ref, e_ref, xo, wo, eo, ready,
    local, xsend, xrecv, dsend, drecv, wsend, wrecv, fsend, frecv, esend, erecv,
):
    s, t, f = lax.axis_index("sp"), lax.axis_index("tp"), lax.axis_index("fs")
    rows, feats = x_ref.shape
    depth = q_ref.shape[0]
    quarter = depth // nf
    some = rows // cut

    def slot(b, c, i):
        return xo.at[pl.ds(b * rows + i * some, some), pl.ds(pl.multiple_of(c * feats, feats), feats)]

    def piece(p, g):
        return wo.at[pl.ds(p * depth + g * quarter, quarter)]

    ring = [lax.rem(s + k, n) for k in range(1, n)]
    mates = [lax.rem(t + k, m) for k in range(1, m)]
    planes = [lax.rem(f + k, nf) for k in range(1, nf)]
    barrier = pltpu.get_barrier_semaphore()
    peers = [{"sp": p} for p in ring] + [{"tp": c} for c in mates] + [{"fs": g} for g in planes]
    for where in peers:
        pl.semaphore_signal(barrier, inc=1, device_id=where, device_id_type=MESH)
    own_x = pltpu.make_async_copy(
        x_ref, xo.at[pl.ds(s * rows, rows), pl.ds(pl.multiple_of(t * feats, feats), feats)], local.at[0]
    )
    own_e = pltpu.make_async_copy(e_ref, eo.at[s], local.at[2])
    own_x.start()
    own_e.start()
    for p in range(n):
        ready[p] = jnp.concatenate(
            [pick_lanes(ref, p, ref.shape[1] // n) for ref in (q_ref, k_ref, pv_ref, pg_ref, v_ref)], axis=1
        )
    own_w = pltpu.make_async_copy(ready.at[s], wo.at[pl.ds(s * depth, depth)], local.at[1])
    pl.semaphore_wait(barrier, len(peers))

    def along(k, way, i):
        b = s - k if way == 0 else s + k
        src = x_ref.at[pl.ds(i * some, some)] if k == 0 else slot(b, t, i)
        return remote(
            src, slot(b, t, i), xsend.at[way, k, i], xrecv.at[way, k, i], {"sp": s + 1 if way == 0 else s - 1}
        )

    def sends(k, way):
        return (s - k >= 0) & (s < n - 1) if way == 0 else (s + k < n) & (s > 0)

    def gets(k, way):
        return s - 1 - k >= 0 if way == 0 else s + 1 + k < n

    def across(index, j, b, i):
        src = x_ref.at[pl.ds(i * some, some)] if index == 0 else slot(b, t, i)
        return remote(src, slot(b, t, i), dsend.at[index, j, i], drecv.at[index, j, i], {"tp": mates[j]})

    def across_in(index, j, b, i):
        c = lax.rem(t + m - 1 - j, m)
        return remote(slot(b, c, i), slot(b, c, i), dsend.at[index, j, i], drecv.at[index, j, i], {"tp": mates[j]})

    started = []
    for k in range(1, n):
        p = ring[k - 1]
        started.append(
            remote(
                ready.at[p, pl.ds(f * quarter, quarter)], piece(s, f), wsend.at[k - 1], wrecv.at[k - 1], {"sp": p}
            )
        )
        started.append(remote(e_ref, eo.at[s], esend.at[k - 1], erecv.at[k - 1], {"sp": p}))
    for copy in started:
        copy.start()
    for i in range(cut):
        for way in range(2):
            @pl.when(sends(0, way))
            def _():
                along(0, way, i).start()
    for i in range(cut):
        for j in range(m - 1):
            across(0, j, s, i).start()
    own_w.start()
    for k in range(1, n):
        p = lax.rem(s + n - k, n)
        remote(piece(p, f), piece(p, f), wsend.at[k - 1], wrecv.at[k - 1], {"sp": p}).wait_recv()
        for g in range(nf - 1):
            copy = remote(piece(p, f), piece(p, f), fsend.at[k - 1, g], frecv.at[k - 1, g], {"fs": planes[g]})
            copy.start()
            started.append(copy)
    for k in range(n - 1):
        for i in range(cut):
            for way in range(2):
                @pl.when(gets(k, way))
                def _():
                    b = s - 1 - k if way == 0 else s + 1 + k
                    remote(
                        slot(b, t, i), slot(b, t, i), xsend.at[way, k, i], xrecv.at[way, k, i], {"sp": b}
                    ).wait_recv()
                    if k + 1 < n - 1:
                        @pl.when(sends(k + 1, way))
                        def _():
                            along(k + 1, way, i).start()
                    for j in range(m - 1):
                        across(1 + 2 * k + way, j, b, i).start()
    for i in range(cut):
        for j in range(m - 1):
            across_in(0, j, s, i).wait_recv()
            across(0, j, s, i).wait_send()
    for k in range(n - 1):
        for way in range(2):
            @pl.when(gets(k, way))
            def _():
                b = s - 1 - k if way == 0 else s + 1 + k
                for i in range(cut):
                    for j in range(m - 1):
                        across_in(1 + 2 * k + way, j, b, i).wait_recv()
                        across(1 + 2 * k + way, j, b, i).wait_send()

            @pl.when(sends(k, way))
            def _():
                for i in range(cut):
                    along(k, way, i).wait_send()
    for k in range(1, n):
        p = lax.rem(s + n - k, n)
        remote(eo.at[p], eo.at[p], esend.at[k - 1], erecv.at[k - 1], {"sp": p}).wait_recv()
        for g in range(nf - 1):
            source = lax.rem(f + nf - 1 - g, nf)
            remote(
                piece(p, source), piece(p, source), fsend.at[k - 1, g], frecv.at[k - 1, g], {"fs": source}
            ).wait_recv()
    for copy in started:
        copy.wait_send()
    for copy in (own_x, own_w, own_e):
        copy.wait()


def collect(n, m, nf, x, parts, e):
    rows, feats = x.shape
    vmem = pl.BlockSpec(memory_space=pltpu.VMEM)
    dma = pltpu.SemaphoreType.DMA
    hops, mates, planes, cut = max(n - 1, 1), max(m - 1, 1), max(nf - 1, 1), 2
    depth, wide = parts[0].shape[0], sum(part.shape[1] for part in parts) // n
    return pl.pallas_call(
        functools.partial(collect_kernel, n, m, nf, cut),
        out_shape=(
            jax.ShapeDtypeStruct((n * rows, m * feats), bf16),
            jax.ShapeDtypeStruct((n * depth, wide), bf16),
            jax.ShapeDtypeStruct((n,) + e.shape, f32),
        ),
        in_specs=[vmem] * 7,
        out_specs=(vmem,) * 3,
        scratch_shapes=[
            pltpu.VMEM((n, depth, wide), bf16),
            dma((3,)),
            dma((2, hops, cut)), dma((2, hops, cut)),
            dma((2 * n - 1, mates, cut)), dma((2 * n - 1, mates, cut)),
            dma((hops,)), dma((hops,)),
            dma((hops, planes)), dma((hops, planes)),
            dma((hops,)), dma((hops,)),
        ],
        compiler_params=pltpu.CompilerParams(collective_id=0, has_side_effects=True),
    )(x, *parts, e)


def pick(ref, s, n, width):
    out = ref[:, :width]
    for i in range(1, n):
        out = jnp.where(s == i, ref[:, i * width : (i + 1) * width], out)
    return out


def mix_kernel(
    n, m, hc, cc, rows,
    x_ref, gain_ref, w_ref, e_ref, dd_ref, du_ref, db_ref, cd_ref, cu_ref, cb_ref, hs_ref, st_ref, taps_ref,
    mix_ref, conv_ref, sums_ref,
    proj, low, glu, maps, adds, qe, oi, states,
):
    s = lax.axis_index("sp")
    heads = hc // GROUP
    length = x_ref.shape[0]
    feats = x_ref.shape[1]
    block = 256 if length % 256 == 0 else rows

    @pl.loop(0, length // block)
    def _(i):
        at = pl.ds(pl.multiple_of(i * block, block), block)
        x = x_ref[at, :].astype(f32)
        normed = (x * lax.rsqrt(jnp.mean(x * x, axis=-1, keepdims=True) + 1e-06) * gain_ref[...]).astype(bf16)
        proj[at, :] = dot1(normed, w_ref[...])
        low[0, at, :] = jnp.tanh(dot1(normed, dd_ref[...])).astype(bf16)
        low[1, at, :] = dot1(normed, cd_ref[...]).astype(bf16)

    reach = taps_ref.shape[0] // 2
    top = 16 * ((reach + 15) // 16)
    glu[pl.ds(0, top), :] = jnp.zeros((top, cc), f32)
    glu[pl.ds(top + length, top), :] = jnp.zeros((top, cc), f32)
    base = 2 * hc
    gate = proj[:, base + cc : base + 2 * cc]
    glu[pl.ds(top, length), :] = (proj[:, base : base + cc] * jax.nn.sigmoid(gate)).astype(bf16).astype(f32)
    taps = pick(taps_ref, s, n, cc)
    step = 64
    for r in range(0, length, step):
        total = jnp.zeros((step, cc), f32)
        for j in range(taps_ref.shape[0]):
            total += taps[j : j + 1, :] * glu[pl.ds(r + top - reach + j, step), :]
        conv_ref[pl.ds(r, step), :] = total
    ones = jnp.ones((8, cc), f32)
    conv = conv_ref[...]
    row = lax.broadcasted_iota(jnp.int32, (8, length), 0)
    first = exact_rows(ones, conv)
    second = exact_rows(ones, conv * conv)
    sums_ref[...] = jnp.where(row == 0, first, jnp.where(row == 1, second, 0.0))

    size = 2 * CHUNK if rows % (2 * CHUNK) == 0 else CHUNK
    per = size // CHUNK
    ti = lax.broadcasted_iota(jnp.int32, (size, size), 0)
    tj = lax.broadcasted_iota(jnp.int32, (size, size), 1)
    same = ti // CHUNK == tj // CHUNK
    whole = same.astype(f32).astype(bf16)
    eye = (ti == tj).astype(f32)
    small_eye = (
        lax.broadcasted_iota(jnp.int32, (GROUP, GROUP), 0) == lax.broadcasted_iota(jnp.int32, (GROUP, GROUP), 1)
    ).astype(f32)
    du, cu = pick(du_ref, s, n, hc), pick(cu_ref, s, n, hc)
    db, cb = pick(db_ref, s, n, hc), pick(cb_ref, s, n, hc)
    hs = pick(hs_ref, s, n, hc)
    local_heads = e_ref.shape[1] // 2
    erow = lax.broadcasted_iota(jnp.int32, (2 * local_heads, GROUP), 0)

    for h in range(heads):
        lanes = slice(h * GROUP, (h + 1) * GROUP)
        klanes = slice(hc + h * GROUP, hc + (h + 1) * GROUP)
        vlanes = slice(base + 2 * cc + h * GROUP, base + 2 * cc + (h + 1) * GROUP)
        pick_offset = (erow == s * heads + h).astype(f32)
        pick_extra = (erow == local_heads + s * heads + h).astype(f32)

        @pl.loop(0, length // size)
        def _(i):
            at = pl.ds(pl.multiple_of(i * size, size), size)
            inner = rows // size
            if inner == 1:
                entry = e_ref[i]
            else:
                entry = e_ref[i // inner, :, pl.ds(pl.multiple_of((i % inner) * size, size), size)]
            offset = lax.dot_general(entry, pick_offset, TN, precision=lax.Precision.HIGHEST, preferred_element_type=f32)
            extra = lax.dot_general(entry, pick_extra, TN, precision=lax.Precision.HIGHEST, preferred_element_type=f32)
            pre = db[:, lanes] + dot1(low[0, at, :], du[:, lanes]) + offset
            lw = -jnp.exp(-jax.nn.softplus(-pre) - 0.5) + extra
            rate = jax.nn.sigmoid(cb[:, lanes] + dot1(low[1, at, :], cu[:, lanes]))
            q = proj[at, lanes].astype(bf16).astype(f32)
            k = proj[at, klanes].astype(bf16).astype(f32)
            vb = proj[at, vlanes].astype(bf16)
            unit = k * lax.rsqrt(jnp.sum(k * k, axis=-1, keepdims=True) + 1e-06)
            rated = unit * rate
            total = exact_left(whole, lw)
            for d in range(2):
                strict = same & ((ti > tj) if d == 0 else (ti < tj))
                upto = same & ((ti >= tj) if d == 0 else (ti <= tj))
                g = exact_left(upto.astype(f32).astype(bf16), lw)
                before = g - lw
                middle = 0.5 * total
                ahead = jnp.exp(middle - g)
                left = halves(jnp.concatenate([unit * jnp.exp(before - middle), q * jnp.exp(g - middle)], axis=0))
                right = halves(jnp.concatenate([rated * ahead, k * ahead], axis=0))
                scores = dot3(left, right, NT)
                a_ur = jnp.where(strict, scores[:size, :size], 0.0)
                a_uk = jnp.where(strict, scores[:size, size:], 0.0)
                a_qr = jnp.where(upto, scores[size:, :size], 0.0)
                a_qk = jnp.where(upto, scores[size:, size:], 0.0)
                width = 1
                inverse = eye - jnp.where((ti // 2 == tj // 2), a_ur, 0.0)
                width = 2
                while width < CHUNK:
                    part = jnp.where(
                        (ti // (2 * width) == tj // (2 * width)) & (ti // width != tj // width), a_ur, 0.0
                    )
                    pair = halves(inverse)
                    inverse = inverse - dot3(dot3(pair, part), pair)
                    width *= 2
                a_kv = halves(jnp.concatenate([a_uk, a_qk], axis=0))
                both = dot1(a_kv[0], vb) + dot1(a_kv[1], vb)
                wy = dot3(inverse, jnp.concatenate([unit * jnp.exp(before), both[:size]], axis=1))
                far = dot3(a_qr, wy)
                qe[d, at, :] = q * jnp.exp(g) - far[:, :GROUP]
                oi[d, at, :] = both[size:] - far[:, GROUP:]
                tail = jnp.exp(total - g)
                r_end, k_end = rated * tail, k * tail
                for c in range(per):
                    cut = slice(c * CHUNK, (c + 1) * CHUNK)
                    moved = dot3(wy[cut], r_end[cut], TN)
                    ke = halves(k_end[cut])
                    came = dot1(vb[cut], ke[0], TN) + dot1(vb[cut], ke[1], TN)
                    decay = jnp.exp(total[c * CHUNK : c * CHUNK + 1])
                    maps[d, i * per + c] = small_eye * decay - moved[:GROUP]
                    adds[d, i * per + c] = came - moved[GROUP:]

        chunks = length // CHUNK
        now = [st_ref[0, 0, s * heads + h], st_ref[0, 1, s * heads + h]]
        for c in range(chunks):
            for d in range(2):
                at = c if d == 0 else chunks - 1 - c
                states[d, at] = now[d]
                if c < chunks - 1:
                    now[d] = dot3(now[d], maps[d, at]) + adds[d, at]
        share = rows // m
        for c in range(chunks):
            cut = pl.ds(c * CHUNK, CHUNK)
            out = oi[0, cut, :] + oi[1, cut, :]
            for d in range(2):
                out += dot3(qe[d, cut, :], states[d, c], NT)
            centered = out - jnp.mean(out, axis=-1, keepdims=True)
            power = jnp.mean(centered * centered, axis=-1, keepdims=True)
            done = (centered * lax.rsqrt(power + 0.00064) * hs[:, lanes]).astype(bf16)
            for piece in range(0, CHUNK, min(share, CHUNK)):
                token = c * CHUNK + piece
                take = min(share, CHUNK)
                owner, inside = token // rows, token % rows
                mix_ref[inside // share, pl.ds(owner * share + inside % share, take), lanes] = done[piece : piece + take]


def exact_rows(ones, x):
    return lax.dot_general(ones, x, NT, precision=lax.Precision.HIGHEST, preferred_element_type=f32)


def mix(n, m, hc, cc, rows, *args):
    length = args[0].shape[0]
    vmem = pl.BlockSpec(memory_space=pltpu.VMEM)
    rank = args[4].shape[1]
    reach = args[12].shape[0] // 2
    top = 16 * ((reach + 15) // 16)
    chunks = length // CHUNK
    return pl.pallas_call(
        functools.partial(mix_kernel, n, m, hc, cc, rows),
        out_shape=(
            jax.ShapeDtypeStruct((m, length // m, hc), bf16),
            jax.ShapeDtypeStruct((length, cc), f32),
            jax.ShapeDtypeStruct((8, length), f32),
        ),
        in_specs=[vmem] * len(args),
        out_specs=(vmem,) * 3,
        scratch_shapes=[
            pltpu.VMEM((length, args[2].shape[1]), f32),
            pltpu.VMEM((2, length, rank), bf16),
            pltpu.VMEM((length + 2 * top, cc), f32),
            pltpu.VMEM((2, chunks, GROUP, GROUP), f32),
            pltpu.VMEM((2, chunks, GROUP, GROUP), f32),
            pltpu.VMEM((2, length, GROUP), f32),
            pltpu.VMEM((2, length, GROUP), f32),
            pltpu.VMEM((2, chunks, GROUP, GROUP), f32),
        ],
    )(*args)


def output_kernel(
    n, m, hc, cc, pack,
    mix_ref, conv_ref, sums_ref, cs_ref, wm_ref, wc_ref, out_ref,
    own, around, mates_act, sums_in, wm_in, wc_in, total, block,
    local, ssend, srecv, vsend, vrecv, asend, arecv, dsend, drecv, osend, orecv,
):
    s, t = lax.axis_index("sp"), lax.axis_index("tp")
    here = s * m + t
    everyone = n * m
    length = conv_ref.shape[0]
    half = length // m
    share = half // n
    columns = wm_ref.shape[1]
    packed = half // pack
    mates = [lax.rem(t + k, m) for k in range(1, m)]

    def other(k):
        p = lax.rem(here + k, everyone)
        return {"sp": p // m, "tp": p % m}

    greet([other(k) for k in range(1, everyone)])
    outs = []
    for k in range(1, everyone):
        outs.append(remote(sums_ref, sums_in.at[k - 1], ssend.at[k - 1], srecv.at[k - 1], other(k)))
    for j in range(m - 1):
        outs.append(remote(wm_ref, wm_in.at[j], vsend.at[0, j], vrecv.at[0, j], {"tp": mates[j]}))
        outs.append(remote(wc_ref, wc_in.at[j], vsend.at[1, j], vrecv.at[1, j], {"tp": mates[j]}))
    for copy in outs:
        copy.start()
    width = mix_ref.shape[2]
    for c in range(m):
        for i in range(pack):
            own[c, pl.ds(0, packed), pl.ds(i * hc, hc)] = mix_ref[c, pl.ds(i * packed, packed), :]
    pieces = m + 1

    def slab(ref, i):
        if i == 0:
            return ref.at[:, pl.ds(0, packed)]
        return ref.at[lax.rem(t + i, m), pl.ds(packed, half)]

    def along(k, way, i):
        b = s - k if way == 0 else s + k
        src = slab(own if k == 0 else around.at[b], i)
        return remote(
            src, slab(around.at[b], i), asend.at[way, k, i], arecv.at[way, k, i], {"sp": s + 1 if way == 0 else s - 1}
        )

    def sends(k, way):
        return (s - k >= 0) & (s < n - 1) if way == 0 else (s + k < n) & (s > 0)

    def gets(k, way):
        return s - 1 - k >= 0 if way == 0 else s + 1 + k < n

    def across(index, j, b, i):
        at = pl.ds(0, packed) if i == 0 else pl.ds(packed, half)
        src = own.at[mates[j], at] if index == 0 else around.at[b, mates[j], at]
        return remote(src, mates_act.at[j, b, at], dsend.at[index, j, i], drecv.at[index, j, i], {"tp": mates[j]})

    def add(b, act, wm, wc):
        w = wm[pl.ds(pl.multiple_of(b * hc, hc), hc), :]
        for i in range(pack):
            rows = pl.ds(i * packed, packed)
            total[rows, :] += dot1(act[pl.ds(0, packed), pl.ds(i * hc, hc)], w)
        total[...] += dot1(act[pl.ds(packed, half), :], wc[pl.ds(pl.multiple_of(b * cc, cc), cc), :])

    def pass_on(k, i):
        for way in range(2):
            @pl.when(gets(k, way))
            def _():
                b = s - 1 - k if way == 0 else s + 1 + k
                part = slab(around.at[b], i)
                remote(part, part, asend.at[way, k, i], arecv.at[way, k, i], {"sp": b}).wait_recv()
                if k + 1 < n - 1:
                    @pl.when(sends(k + 1, way))
                    def _():
                        along(k + 1, way, i).start()
                if i == 0:
                    for j in range(m - 1):
                        across(1 + 2 * k + way, j, b, 0).start()
                elif i < m:
                    across(1 + 2 * k + way, i - 1, b, 1).start()

    def begin(i):
        for way in range(2):
            @pl.when(sends(0, way))
            def _():
                along(0, way, i).start()

    begin(0)
    for j in range(m - 1):
        across(0, j, s, 0).start()
    for copy in outs[: everyone - 1]:
        copy.wait()
    stats = sums_ref[...]
    for k in range(everyone - 1):
        stats += sums_in[k]
    row = lax.broadcasted_iota(jnp.int32, (8, cc), 0)
    channels = cc * n * m

    def spread(which):
        return lax.dot_general(
            stats, (row == which).astype(f32), TN, precision=lax.Precision.HIGHEST, preferred_element_type=f32
        )

    mean = spread(0) / channels
    power = spread(1) / channels - mean * mean
    gain = pick(cs_ref, s, n, cc)
    done = jax.nn.silu((conv_ref[...] - mean) * lax.rsqrt(power + 1e-05) * gain).astype(bf16)
    for token in range(0, length, share):
        unit = token // share
        own[unit % m, pl.ds(packed + (unit // m) * share, share), :] = done[token : token + share]

    for i in range(1, pieces):
        begin(i)
    for j in range(m - 1):
        across(0, j, s, 1).start()
    total[...] = jnp.zeros_like(total)
    pass_on(0, 0)
    add(s, own.at[t], wm_ref, wc_ref)
    for copy in outs[everyone - 1 :]:
        copy.wait()

    def from_mates(index, b):
        for j in range(m - 1):
            for i in range(2):
                across(index, j, b, i).wait_recv()
            add(b, mates_act.at[j, b], wm_in.at[j], wc_in.at[j])
            for i in range(2):
                across(index, j, b, i).wait_send()

    for k in range(n - 1):
        if k > 0:
            pass_on(k, 0)
        for i in range(1, pieces):
            pass_on(k, i)
        for way in range(2):
            @pl.when(gets(k, way))
            def _():
                b = s - 1 - k if way == 0 else s + 1 + k
                add(b, around.at[b, t], wm_ref, wc_ref)
        if k == 0:
            from_mates(0, s)
        else:
            for way in range(2):
                @pl.when(gets(k - 1, way))
                def _():
                    from_mates(2 * k - 1 + way, s - k if way == 0 else s + k)
    for way in range(2):
        @pl.when(gets(n - 2, way))
        def _():
            from_mates(2 * n - 3 + way, s - n + 1 if way == 0 else s + n - 1)
    for k in range(n - 1):
        for way in range(2):
            @pl.when(sends(k, way))
            def _():
                for i in range(pieces):
                    along(k, way, i).wait_send()
    block[...] = total[...].astype(bf16)
    mine = out_ref.at[:, pl.ds(pl.multiple_of(s * columns, columns), columns)]
    keep = pltpu.make_async_copy(block.at[pl.ds(s * share, share)], mine, local.at[0])
    keep.start()
    final = []
    for k in range(1, n):
        p = lax.rem(s + k, n)
        copy = remote(block.at[pl.ds(p * share, share)], mine, osend.at[k - 1], orecv.at[k - 1], {"sp": p})
        copy.start()
        final.append(copy)
    for k in range(1, n):
        p = lax.rem(s + n - k, n)
        part = out_ref.at[:, pl.ds(pl.multiple_of(p * columns, columns), columns)]
        remote(part, part, osend.at[k - 1], orecv.at[k - 1], {"sp": p}).wait_recv()
        final[k - 1].wait_send()
    keep.wait()


def output(n, m, hc, cc, mixed, conv, sums, cs, wm, wc):
    length = conv.shape[0]
    half, columns = length // m, wm.shape[1]
    pack = max(cc // hc, 1)
    rows = half // pack + half
    vmem = pl.BlockSpec(memory_space=pltpu.VMEM)
    dma = pltpu.SemaphoreType.DMA
    hops, mates = max(n - 1, 1), max(m - 1, 1)
    return pl.pallas_call(
        functools.partial(output_kernel, n, m, hc, cc, pack),
        out_shape=jax.ShapeDtypeStruct((half // n, n * columns), bf16),
        in_specs=[vmem] * 6,
        out_specs=vmem,
        scratch_shapes=[
            pltpu.VMEM((m, rows, cc), bf16),
            pltpu.VMEM((n, m, rows, cc), bf16),
            pltpu.VMEM((mates, n, rows, cc), bf16),
            pltpu.VMEM((n * m - 1, 8, length), f32),
            pltpu.VMEM((mates,) + wm.shape, bf16),
            pltpu.VMEM((mates,) + wc.shape, bf16),
            pltpu.VMEM((half, columns), f32),
            pltpu.VMEM((half, columns), bf16),
            dma((1,)),
            dma((n * m - 1,)), dma((n * m - 1,)),
            dma((2, mates)), dma((2, mates)),
            dma((2, hops, m + 1)), dma((2, hops, m + 1)),
            dma((2 * n - 1, mates, 2)), dma((2 * n - 1, mates, 2)),
            dma((hops,)), dma((hops,)),
        ],
        compiler_params=pltpu.CompilerParams(collective_id=1, has_side_effects=True),
    )(mixed, conv, sums, cs, wm, wc)


highest = lax.Precision.HIGHEST


def carried_in(x, axis, combine, identity, reverse):
    length, here = (lax.axis_size(axis), lax.axis_index(axis))
    everything = jax.tree.map(
        lambda part, kind: lax.all_gather(part.astype(kind), axis), x, (jnp.bfloat16, jnp.bfloat16)
    )
    start = jax.tree.map(
        lambda part, zero: jnp.broadcast_to(jnp.asarray(zero, part.dtype), part.shape), x, identity
    )

    def hop(k, before):
        at = length - 1 - k if reverse else k
        reached = at > here if reverse else at < here
        new = combine(
            before, jax.tree.map(lambda part, own: part[at].astype(own.dtype), everything, x)
        )
        return jax.tree.map(lambda a, b: jnp.where(reached, a, b), new, before)

    return lax.fori_loop(0, length, hop, start)


def padded_2(block, sides, width):
    for axis, dim in sides:
        count = lax.axis_size(axis)
        forward = [(i, i + 1) for i in range(count - 1)]
        backward = [(target, source) for source, target in forward]
        low = lax.ppermute(
            lax.slice_in_dim(block, block.shape[dim] - width, None, axis=dim), axis, forward
        )
        high = lax.ppermute(lax.slice_in_dim(block, 0, width, axis=dim), axis, backward)
        block = jnp.concatenate([low, block, high], axis=dim)
    return block


def split_heads(values):
    return values.reshape(values.shape[0], -1, GROUP)


def paired(values):
    return jnp.stack([values, jnp.flip(values, 0)], 1)


def local_step(stacked, inputs):
    fading_multiplier, unit_key, rated_key, keys, values, query = inputs
    projected = jnp.einsum("dhvk,dhk->dhv", stacked, unit_key, precision=highest)
    outer = values[..., None] * keys[:, :, None, :]
    added = jnp.concatenate([jnp.zeros_like(outer), outer], axis=2)
    stacked = (
        stacked * fading_multiplier[:, :, None, :]
        - projected[..., None] * rated_key[:, :, None, :]
        + added
    )
    return (stacked, jnp.einsum("dhvk,dhk->dhv", stacked, query, precision=highest))


def chain_pair(earlier, later):
    product = jnp.einsum("hij,hjk->hik", earlier[0], later[0], precision=highest)
    moved = jnp.einsum("hij,hjk->hik", earlier[1], later[0], precision=highest) + later[1]
    return (product, moved)


def carry_in(initial_memory_matrix, prefix):
    return (
        jnp.einsum("hij,hjk->hik", initial_memory_matrix, prefix[0], precision=highest) + prefix[1]
    )


def head_norm(summed, head_norm_scale):
    centered = summed - jnp.mean(summed, axis=-1, keepdims=True)
    scaled = centered * lax.rsqrt(jnp.mean(centered * centered, axis=-1, keepdims=True) + 0.00064)
    return (
        (scaled * head_norm_scale.reshape(-1, GROUP))
        .reshape(summed.shape[0], -1)
        .astype(jnp.bfloat16)
    )


def rounded(total):
    return lax.optimization_barrier(total.astype(jnp.bfloat16)).astype(jnp.float32)


def mixer_branch(
    normed,
    sums,
    decay_down_weight,
    decay_up_weight,
    decay_bias_base,
    decay_position_offset,
    extra_log_decay,
    correction_down_weight,
    correction_up_weight,
    correction_rate_bias,
    head_norm_scale,
    starting_states,
):
    query = rounded(sums[0])
    keys = rounded(sums[1])
    values = rounded(sums[2])
    low_decay = jnp.tanh(
        jnp.dot(normed, decay_down_weight, preferred_element_type=jnp.float32)
    ).astype(jnp.bfloat16)
    fading_raw_scores = (
        decay_bias_base
        + jnp.dot(low_decay, decay_up_weight, preferred_element_type=jnp.float32)
        + jnp.repeat(decay_position_offset[0], GROUP, axis=1)
    )
    fading_multiplier = jnp.exp(
        -jnp.exp(-jax.nn.softplus(-fading_raw_scores) - 0.5)
        + jnp.repeat(extra_log_decay[0], GROUP, axis=1)
    )
    low_rate = jnp.dot(normed, correction_down_weight, preferred_element_type=jnp.float32).astype(
        jnp.bfloat16
    )
    rate = jax.nn.sigmoid(
        correction_rate_bias
        + jnp.dot(low_rate, correction_up_weight, preferred_element_type=jnp.float32)
    )
    key_heads = split_heads(keys)
    unit_key = key_heads * lax.rsqrt(jnp.sum(key_heads * key_heads, axis=-1, keepdims=True) + 1e-06)
    rated_key = unit_key * split_heads(rate)
    steps = tuple(
        (
            paired(item)
            for item in (
                split_heads(fading_multiplier),
                unit_key,
                rated_key,
                key_heads,
                split_heads(values),
                split_heads(query),
            )
        )
    )
    heads_here = key_heads.shape[1]
    identity = jnp.broadcast_to(
        jnp.eye(GROUP, dtype=jnp.float32),
        (2, heads_here, GROUP, GROUP),
    )
    nothing = jnp.zeros((2, heads_here, GROUP, GROUP), jnp.float32)
    start = jnp.concatenate([identity, nothing], axis=2)
    ends, emitted = lax.scan(local_step, start, steps, unroll=8)
    transfer = ends[:, :, :GROUP]
    alone = ends[:, :, GROUP:]
    through = emitted[..., :GROUP]
    own_part = emitted[..., GROUP:]
    before = carried_in((transfer[0], alone[0]), "sp", chain_pair, (identity[0], nothing[0]), False)
    after = carried_in((transfer[1], alone[1]), "sp", chain_pair, (identity[1], nothing[1]), True)
    starts = jnp.stack(
        [carry_in(starting_states[0, 0], before), carry_in(starting_states[0, 1], after)], 0
    )
    outputs = jnp.einsum("dhvk,tdhk->tdhv", starts, through, precision=highest) + own_part
    summed = outputs[:, 0] + jnp.flip(outputs[:, 1], 0)
    return head_norm(summed, head_norm_scale)


def conv_branch(sums, depthwise_taps_weight, channel_norm_scale):
    glu = (sums[0] * jax.nn.sigmoid(sums[1])).astype(jnp.bfloat16)
    reach = depthwise_taps_weight.shape[0] // 2
    padded = padded_2(glu, (("sp", 0),), reach)
    conv = lax.conv_general_dilated(
        padded.astype(jnp.float32)[None],
        depthwise_taps_weight[:, None, :],
        (1,),
        "VALID",
        dimension_numbers=("NWC", "WIO", "NWC"),
        feature_group_count=depthwise_taps_weight.shape[1],
        precision=highest,
    )[0]
    first, second = lax.psum((jnp.sum(conv, axis=-1), jnp.sum(conv * conv, axis=-1)), "tp")
    width = conv.shape[1] * lax.axis_size("tp")
    mean = first / width
    power = second / width - mean * mean
    return jax.nn.silu(
        (conv - mean[:, None]) * lax.rsqrt(power[:, None] + 1e-05) * channel_norm_scale
    ).astype(jnp.bfloat16)


def spread_device(
    inputs,
    input_norm_scale,
    query_matrix,
    key_matrix,
    value_matrix,
    decay_down_weight,
    decay_up_weight,
    decay_bias_base,
    decay_position_offset,
    extra_log_decay,
    correction_down_weight,
    correction_up_weight,
    correction_rate_bias,
    head_norm_scale,
    starting_states,
    pointwise_value_weight,
    pointwise_gate_weight,
    depthwise_taps_weight,
    channel_norm_scale,
    mixer_output_weight,
    convolution_output_weight,
):
    symbol_vectors = lax.all_gather(inputs[0], "tp", axis=1, tiled=True)
    as_float = symbol_vectors.astype(jnp.float32)
    normed = (
        as_float
        * lax.rsqrt(jnp.mean(as_float * as_float, axis=-1, keepdims=True) + 1e-06)
        * input_norm_scale
    ).astype(jnp.bfloat16)
    mixer_args = (
        decay_down_weight,
        decay_up_weight,
        decay_bias_base,
        decay_position_offset,
        extra_log_decay,
        correction_down_weight,
        correction_up_weight,
        correction_rate_bias,
        head_norm_scale,
        starting_states,
    )
    pieces = (
        lax.all_gather(query_matrix, "sp", axis=0, tiled=True),
        lax.all_gather(key_matrix, "sp", axis=0, tiled=True),
        lax.all_gather(value_matrix, "sp", axis=0, tiled=True),
        lax.all_gather(pointwise_value_weight, "sp", axis=0, tiled=True),
        lax.all_gather(pointwise_gate_weight, "sp", axis=0, tiled=True),
    )
    sums = tuple((jnp.dot(normed, piece, preferred_element_type=jnp.float32) for piece in pieces))
    mixer_out = mixer_branch(normed, sums[:3], *mixer_args)
    conv_out = conv_branch(sums[3:], depthwise_taps_weight, channel_norm_scale)
    joined = jnp.concatenate([mixer_out, conv_out], axis=1)
    weight_rows = jnp.concatenate([mixer_output_weight, convolution_output_weight], axis=0)
    columns = lax.all_gather(weight_rows, "sp", axis=1, tiled=True)
    moved = lax.all_to_all(joined, "tp", split_axis=0, concat_axis=1, tiled=True)
    every_row = lax.all_gather(columns, "tp", axis=0, tiled=True)
    total = jnp.dot(moved, every_row, preferred_element_type=jnp.float32)
    return total.astype(jnp.bfloat16)[None]


def per_device(
    inputs, input_norm_scale, query_matrix, key_matrix, value_matrix,
    decay_down_weight, decay_up_weight, decay_bias_base, decay_position_offset, extra_log_decay,
    correction_down_weight, correction_up_weight, correction_rate_bias, head_norm_scale, starting_states,
    pointwise_value_weight, pointwise_gate_weight, depthwise_taps_weight, channel_norm_scale,
    mixer_output_weight, convolution_output_weight,
):
    n, m, nf = lax.axis_size("sp"), lax.axis_size("tp"), lax.axis_size("fs")
    lanes = query_matrix.shape[1] % (n * GROUP) or pointwise_value_weight.shape[1] % (n * 128)
    if lanes or query_matrix.shape[0] % (nf * 16):
        return spread_device(
            inputs, input_norm_scale, query_matrix, key_matrix, value_matrix,
            decay_down_weight, decay_up_weight, decay_bias_base, decay_position_offset, extra_log_decay,
            correction_down_weight, correction_up_weight, correction_rate_bias, head_norm_scale, starting_states,
            pointwise_value_weight, pointwise_gate_weight, depthwise_taps_weight, channel_norm_scale,
            mixer_output_weight, convolution_output_weight,
        )
    x = inputs[0]
    rows = x.shape[0]
    hc, cc = query_matrix.shape[1] // n, pointwise_value_weight.shape[1] // n
    parts = [query_matrix, key_matrix, pointwise_value_weight, pointwise_gate_weight, value_matrix]
    e = jnp.concatenate([decay_position_offset[0], extra_log_decay[0]], axis=1).T
    everything, columns, shifts = collect(n, m, nf, x, parts, e)
    mixed, conv, sums = mix(
        n, m, hc, cc, rows,
        everything, input_norm_scale[None], columns, shifts,
        decay_down_weight, decay_up_weight, decay_bias_base[None],
        correction_down_weight, correction_up_weight, correction_rate_bias[None],
        head_norm_scale[None], starting_states, depthwise_taps_weight,
    )
    return output(
        n, m, hc, cc, mixed, conv, sums, channel_norm_scale[None], mixer_output_weight, convolution_output_weight
    )[None]


def solution(mesh):
    return jax.shard_map(
        per_device,
        mesh=mesh,
        in_specs=(
            P("fs", "sp", "tp"),
            P(),
            P("sp", "tp"),
            P("sp", "tp"),
            P("sp", "tp"),
            P(),
            P(None, "tp"),
            P("tp"),
            P("fs", "sp", "tp"),
            P("fs", "sp", "tp"),
            P(),
            P(None, "tp"),
            P("tp"),
            P("tp"),
            P("fs", None, "tp", None, None),
            P("sp", "tp"),
            P("sp", "tp"),
            P(None, "tp"),
            P("tp"),
            P("tp", "sp"),
            P("tp", "sp"),
        ),
        out_specs=P("fs", ("sp", "tp"), None),
        check_vma=False,
    )
```

```python
import functools

import jax
import jax.numpy as jnp
from jax import lax
from jax.experimental import pallas as pl
from jax.experimental.pallas import tpu as pltpu
from jax.sharding import PartitionSpec as P

GROUP = 64
CHUNK = 64
MESH = pl.DeviceIdType.MESH
f32 = jnp.float32
bf16 = jnp.bfloat16
NN = (((1,), (0,)), ((), ()))
NT = (((1,), (1,)), ((), ()))
TN = (((0,), (0,)), ((), ()))


def dot1(a, b, dims=NN):
    return lax.dot_general(a, b, dims, preferred_element_type=f32)


def halves(a):
    hi = a.astype(bf16)
    return hi, (a - hi.astype(f32)).astype(bf16)


def dot3(a, b, dims=NN):
    a, b = (x if isinstance(x, tuple) else halves(x) for x in (a, b))
    return dot1(a[0], b[0], dims) + (dot1(a[0], b[1], dims) + dot1(a[1], b[0], dims))


def exact_left(mask, x):
    hi, rest = x.astype(bf16), x - x.astype(bf16).astype(f32)
    mid, low = halves(rest)
    return dot1(mask, hi) + (dot1(mask, mid) + dot1(mask, low))


def remote(src, dst, send, recv, where):
    return pltpu.make_async_remote_copy(
        src_ref=src, dst_ref=dst, send_sem=send, recv_sem=recv, device_id=where, device_id_type=MESH
    )


def greet(peers):
    barrier = pltpu.get_barrier_semaphore()
    for where in peers:
        pl.semaphore_signal(barrier, inc=1, device_id=where, device_id_type=MESH)
    pl.semaphore_wait(barrier, len(peers))


def pick_lanes(ref, p, width):
    return ref[:, p * width : (p + 1) * width]


def collect_kernel(
    n, m, nf, cut,
    x_ref, q_ref, k_ref, pv_ref, pg_ref, v_ref, e_ref, xo, wo, eo, ready,
    local, xsend, xrecv, dsend, drecv, wsend, wrecv, fsend, frecv, esend, erecv,
):
    s, t, f = lax.axis_index("sp"), lax.axis_index("tp"), lax.axis_index("fs")
    rows, feats = x_ref.shape
    depth = q_ref.shape[0]
    quarter = depth // nf
    some = rows // cut

    def slot(b, c, i):
        return xo.at[pl.ds(b * rows + i * some, some), pl.ds(pl.multiple_of(c * feats, feats), feats)]

    def piece(p, g):
        return wo.at[pl.ds(p * depth + g * quarter, quarter)]

    ring = [lax.rem(s + k, n) for k in range(1, n)]
    mates = [lax.rem(t + k, m) for k in range(1, m)]
    planes = [lax.rem(f + k, nf) for k in range(1, nf)]
    barrier = pltpu.get_barrier_semaphore()
    peers = [{"sp": p} for p in ring] + [{"tp": c} for c in mates] + [{"fs": g} for g in planes]
    for where in peers:
        pl.semaphore_signal(barrier, inc=1, device_id=where, device_id_type=MESH)
    own_x = pltpu.make_async_copy(
        x_ref, xo.at[pl.ds(s * rows, rows), pl.ds(pl.multiple_of(t * feats, feats), feats)], local.at[0]
    )
    own_e = pltpu.make_async_copy(e_ref, eo.at[s], local.at[2])
    own_x.start()
    own_e.start()
    for p in range(n):
        ready[p] = jnp.concatenate(
            [pick_lanes(ref, p, ref.shape[1] // n) for ref in (q_ref, k_ref, pv_ref, pg_ref, v_ref)], axis=1
        )
    own_w = pltpu.make_async_copy(ready.at[s], wo.at[pl.ds(s * depth, depth)], local.at[1])
    pl.semaphore_wait(barrier, len(peers))

    def along(k, way, i):
        b = s - k if way == 0 else s + k
        src = x_ref.at[pl.ds(i * some, some)] if k == 0 else slot(b, t, i)
        return remote(
            src, slot(b, t, i), xsend.at[way, k, i], xrecv.at[way, k, i], {"sp": s + 1 if way == 0 else s - 1}
        )

    def sends(k, way):
        return (s - k >= 0) & (s < n - 1) if way == 0 else (s + k < n) & (s > 0)

    def gets(k, way):
        return s - 1 - k >= 0 if way == 0 else s + 1 + k < n

    def across(index, j, b, i):
        src = x_ref.at[pl.ds(i * some, some)] if index == 0 else slot(b, t, i)
        return remote(src, slot(b, t, i), dsend.at[index, j, i], drecv.at[index, j, i], {"tp": mates[j]})

    def across_in(index, j, b, i):
        c = lax.rem(t + m - 1 - j, m)
        return remote(slot(b, c, i), slot(b, c, i), dsend.at[index, j, i], drecv.at[index, j, i], {"tp": mates[j]})

    started = []
    for k in range(1, n):
        p = ring[k - 1]
        started.append(
            remote(
                ready.at[p, pl.ds(f * quarter, quarter)], piece(s, f), wsend.at[k - 1], wrecv.at[k - 1], {"sp": p}
            )
        )
        started.append(remote(e_ref, eo.at[s], esend.at[k - 1], erecv.at[k - 1], {"sp": p}))
    for copy in started:
        copy.start()
    for i in range(cut):
        for way in range(2):
            @pl.when(sends(0, way))
            def _():
                along(0, way, i).start()
    for i in range(cut):
        for j in range(m - 1):
            across(0, j, s, i).start()
    own_w.start()
    for k in range(1, n):
        p = lax.rem(s + n - k, n)
        remote(piece(p, f), piece(p, f), wsend.at[k - 1], wrecv.at[k - 1], {"sp": p}).wait_recv()
        for g in range(nf - 1):
            copy = remote(piece(p, f), piece(p, f), fsend.at[k - 1, g], frecv.at[k - 1, g], {"fs": planes[g]})
            copy.start()
            started.append(copy)
    for k in range(n - 1):
        for i in range(cut):
            for way in range(2):
                @pl.when(gets(k, way))
                def _():
                    b = s - 1 - k if way == 0 else s + 1 + k
                    remote(
                        slot(b, t, i), slot(b, t, i), xsend.at[way, k, i], xrecv.at[way, k, i], {"sp": b}
                    ).wait_recv()
                    if k + 1 < n - 1:
                        @pl.when(sends(k + 1, way))
                        def _():
                            along(k + 1, way, i).start()
                    for j in range(m - 1):
                        across(1 + 2 * k + way, j, b, i).start()
    for i in range(cut):
        for j in range(m - 1):
            across_in(0, j, s, i).wait_recv()
            across(0, j, s, i).wait_send()
    for k in range(n - 1):
        for way in range(2):
            @pl.when(gets(k, way))
            def _():
                b = s - 1 - k if way == 0 else s + 1 + k
                for i in range(cut):
                    for j in range(m - 1):
                        across_in(1 + 2 * k + way, j, b, i).wait_recv()
                        across(1 + 2 * k + way, j, b, i).wait_send()

            @pl.when(sends(k, way))
            def _():
                for i in range(cut):
                    along(k, way, i).wait_send()
    for k in range(1, n):
        p = lax.rem(s + n - k, n)
        remote(eo.at[p], eo.at[p], esend.at[k - 1], erecv.at[k - 1], {"sp": p}).wait_recv()
        for g in range(nf - 1):
            source = lax.rem(f + nf - 1 - g, nf)
            remote(
                piece(p, source), piece(p, source), fsend.at[k - 1, g], frecv.at[k - 1, g], {"fs": source}
            ).wait_recv()
    for copy in started:
        copy.wait_send()
    for copy in (own_x, own_w, own_e):
        copy.wait()


def collect(n, m, nf, x, parts, e):
    rows, feats = x.shape
    vmem = pl.BlockSpec(memory_space=pltpu.VMEM)
    dma = pltpu.SemaphoreType.DMA
    hops, mates, planes, cut = max(n - 1, 1), max(m - 1, 1), max(nf - 1, 1), 2
    depth, wide = parts[0].shape[0], sum(part.shape[1] for part in parts) // n
    return pl.pallas_call(
        functools.partial(collect_kernel, n, m, nf, cut),
        out_shape=(
            jax.ShapeDtypeStruct((n * rows, m * feats), bf16),
            jax.ShapeDtypeStruct((n * depth, wide), bf16),
            jax.ShapeDtypeStruct((n,) + e.shape, f32),
        ),
        in_specs=[vmem] * 7,
        out_specs=(vmem,) * 3,
        scratch_shapes=[
            pltpu.VMEM((n, depth, wide), bf16),
            dma((3,)),
            dma((2, hops, cut)), dma((2, hops, cut)),
            dma((2 * n - 1, mates, cut)), dma((2 * n - 1, mates, cut)),
            dma((hops,)), dma((hops,)),
            dma((hops, planes)), dma((hops, planes)),
            dma((hops,)), dma((hops,)),
        ],
        compiler_params=pltpu.CompilerParams(collective_id=0, has_side_effects=True),
    )(x, *parts, e)


def pick(ref, s, n, width):
    out = ref[:, :width]
    for i in range(1, n):
        out = jnp.where(s == i, ref[:, i * width : (i + 1) * width], out)
    return out


def mix_kernel(
    n, m, hc, cc, rows,
    x_ref, gain_ref, w_ref, e_ref, dd_ref, du_ref, db_ref, cd_ref, cu_ref, cb_ref, hs_ref, st_ref, taps_ref,
    mix_ref, conv_ref, sums_ref,
    proj, low, glu, maps, adds, qe, oi, states,
):
    s = lax.axis_index("sp")
    heads = hc // GROUP
    length = x_ref.shape[0]
    feats = x_ref.shape[1]
    block = 256 if length % 256 == 0 else rows

    @pl.loop(0, length // block)
    def _(i):
        at = pl.ds(pl.multiple_of(i * block, block), block)
        x = x_ref[at, :].astype(f32)
        normed = (x * lax.rsqrt(jnp.mean(x * x, axis=-1, keepdims=True) + 1e-06) * gain_ref[...]).astype(bf16)
        proj[at, :] = dot1(normed, w_ref[...])
        low[0, at, :] = jnp.tanh(dot1(normed, dd_ref[...])).astype(bf16)
        low[1, at, :] = dot1(normed, cd_ref[...]).astype(bf16)

    reach = taps_ref.shape[0] // 2
    top = 16 * ((reach + 15) // 16)
    glu[pl.ds(0, top), :] = jnp.zeros((top, cc), f32)
    glu[pl.ds(top + length, top), :] = jnp.zeros((top, cc), f32)
    base = 2 * hc
    gate = proj[:, base + cc : base + 2 * cc]
    glu[pl.ds(top, length), :] = (proj[:, base : base + cc] * jax.nn.sigmoid(gate)).astype(bf16).astype(f32)
    taps = pick(taps_ref, s, n, cc)
    step = 64
    for r in range(0, length, step):
        total = jnp.zeros((step, cc), f32)
        for j in range(taps_ref.shape[0]):
            total += taps[j : j + 1, :] * glu[pl.ds(r + top - reach + j, step), :]
        conv_ref[pl.ds(r, step), :] = total
    ones = jnp.ones((8, cc), f32)
    conv = conv_ref[...]
    row = lax.broadcasted_iota(jnp.int32, (8, length), 0)
    first = exact_rows(ones, conv)
    second = exact_rows(ones, conv * conv)
    sums_ref[...] = jnp.where(row == 0, first, jnp.where(row == 1, second, 0.0))

    size = 2 * CHUNK if rows % (2 * CHUNK) == 0 else CHUNK
    per = size // CHUNK
    ti = lax.broadcasted_iota(jnp.int32, (size, size), 0)
    tj = lax.broadcasted_iota(jnp.int32, (size, size), 1)
    same = ti // CHUNK == tj // CHUNK
    whole = same.astype(f32).astype(bf16)
    eye = (ti == tj).astype(f32)
    small_eye = (
        lax.broadcasted_iota(jnp.int32, (GROUP, GROUP), 0) == lax.broadcasted_iota(jnp.int32, (GROUP, GROUP), 1)
    ).astype(f32)
    du, cu = pick(du_ref, s, n, hc), pick(cu_ref, s, n, hc)
    db, cb = pick(db_ref, s, n, hc), pick(cb_ref, s, n, hc)
    hs = pick(hs_ref, s, n, hc)
    local_heads = e_ref.shape[1] // 2
    erow = lax.broadcasted_iota(jnp.int32, (2 * local_heads, GROUP), 0)

    for h in range(heads):
        lanes = slice(h * GROUP, (h + 1) * GROUP)
        klanes = slice(hc + h * GROUP, hc + (h + 1) * GROUP)
        vlanes = slice(base + 2 * cc + h * GROUP, base + 2 * cc + (h + 1) * GROUP)
        pick_offset = (erow == s * heads + h).astype(f32)
        pick_extra = (erow == local_heads + s * heads + h).astype(f32)

        together = 2 if (length // size) % 2 == 0 else 1

        def prepare(i):
            at = pl.ds(pl.multiple_of(i * size, size), size)
            inner = rows // size
            if inner == 1:
                entry = e_ref[i]
            else:
                entry = e_ref[i // inner, :, pl.ds(pl.multiple_of((i % inner) * size, size), size)]
            offset = lax.dot_general(entry, pick_offset, TN, precision=lax.Precision.HIGHEST, preferred_element_type=f32)
            extra = lax.dot_general(entry, pick_extra, TN, precision=lax.Precision.HIGHEST, preferred_element_type=f32)
            pre = db[:, lanes] + dot1(low[0, at, :], du[:, lanes]) + offset
            lw = -jnp.exp(-jax.nn.softplus(-pre) - 0.5) + extra
            rate = jax.nn.sigmoid(cb[:, lanes] + dot1(low[1, at, :], cu[:, lanes]))
            q = proj[at, lanes].astype(bf16).astype(f32)
            k = proj[at, klanes].astype(bf16).astype(f32)
            vb = proj[at, vlanes].astype(bf16)
            unit = k * lax.rsqrt(jnp.sum(k * k, axis=-1, keepdims=True) + 1e-06)
            rated = unit * rate
            total = exact_left(whole, lw)
            middle = 0.5 * total
            work = []
            for d in range(2):
                strict = same & ((ti > tj) if d == 0 else (ti < tj))
                upto = same & ((ti >= tj) if d == 0 else (ti <= tj))
                g = exact_left(upto.astype(f32).astype(bf16), lw)
                before = g - lw
                ahead = jnp.exp(middle - g)
                right = halves(jnp.concatenate([rated * ahead, k * ahead], axis=0))
                near = dot3(unit * jnp.exp(before - middle), right, NT)
                seen = dot1((q * jnp.exp(g - middle)).astype(bf16), right[0], NT)
                a_ur = jnp.where(strict, near[:, :size], 0.0)
                a_uk = jnp.where(strict, near[:, size:], 0.0)
                a_qr = jnp.where(upto, seen[:, :size], 0.0).astype(bf16)
                a_qk = jnp.where(upto, seen[:, size:], 0.0).astype(bf16)
                inverse = eye - jnp.where((ti // 2 == tj // 2), a_ur, 0.0)
                work.append((i, d, at, a_ur, a_uk, a_qr, a_qk, inverse, g, before, total, q, k, vb, unit, rated))
            return work

        def finish(item, inverse):
            i, d, at, a_ur, a_uk, a_qr, a_qk, _, g, before, total, q, k, vb, unit, rated = item
            a_uk = halves(a_uk)
            pulled = dot1(a_uk[0], vb) + dot1(a_uk[1], vb)
            wy = dot3(inverse, jnp.concatenate([unit * jnp.exp(before), pulled], axis=1))
            far = dot1(a_qr, wy.astype(bf16))
            qe[d, at, :] = q * jnp.exp(g) - far[:, :GROUP]
            oi[d, at, :] = dot1(a_qk, vb) - far[:, GROUP:]
            tail = jnp.exp(total - g)
            r_end, k_end = rated * tail, k * tail
            for c in range(per):
                cut = slice(c * CHUNK, (c + 1) * CHUNK)
                moved = dot3(wy[cut], r_end[cut], TN)
                ke = halves(k_end[cut])
                came = dot1(vb[cut], ke[0], TN) + dot1(vb[cut], ke[1], TN)
                decay = jnp.exp(total[c * CHUNK : c * CHUNK + 1])
                maps[d, i * per + c] = small_eye * decay - moved[:GROUP]
                adds[d, i * per + c] = came - moved[GROUP:]

        @pl.loop(0, length // size // together)
        def _(step_at):
            work = []
            for u in range(together):
                work += prepare(step_at * together + u)
            inverses = [item[7] for item in work]
            width = 2
            while width < CHUNK:
                level = (ti // (2 * width) == tj // (2 * width)) & (ti // width != tj // width)
                pairs = [halves(x) for x in inverses]
                firsts = [dot3(p, jnp.where(level, item[3], 0.0)) for p, item in zip(pairs, work)]
                inverses = [x - dot3(y, p) for x, y, p in zip(inverses, firsts, pairs)]
                width *= 2
            for item, inverse in zip(work, inverses):
                finish(item, inverse)

        chunks = length // CHUNK
        now = [st_ref[0, 0, s * heads + h], st_ref[0, 1, s * heads + h]]
        for c in range(chunks):
            for d in range(2):
                at = c if d == 0 else chunks - 1 - c
                states[d, at] = now[d]
                if c < chunks - 1:
                    now[d] = dot3(now[d], maps[d, at]) + adds[d, at]
        share = rows // m
        for c in range(chunks):
            cut = pl.ds(c * CHUNK, CHUNK)
            out = oi[0, cut, :] + oi[1, cut, :]
            for d in range(2):
                out += dot3(qe[d, cut, :], states[d, c], NT)
            centered = out - jnp.mean(out, axis=-1, keepdims=True)
            power = jnp.mean(centered * centered, axis=-1, keepdims=True)
            done = (centered * lax.rsqrt(power + 0.00064) * hs[:, lanes]).astype(bf16)
            for piece in range(0, CHUNK, min(share, CHUNK)):
                token = c * CHUNK + piece
                take = min(share, CHUNK)
                owner, inside = token // rows, token % rows
                mix_ref[inside // share, pl.ds(owner * share + inside % share, take), lanes] = done[piece : piece + take]


def exact_rows(ones, x):
    return lax.dot_general(ones, x, NT, precision=lax.Precision.HIGHEST, preferred_element_type=f32)


def mix(n, m, hc, cc, rows, *args):
    length = args[0].shape[0]
    vmem = pl.BlockSpec(memory_space=pltpu.VMEM)
    rank = args[4].shape[1]
    reach = args[12].shape[0] // 2
    top = 16 * ((reach + 15) // 16)
    chunks = length // CHUNK
    return pl.pallas_call(
        functools.partial(mix_kernel, n, m, hc, cc, rows),
        out_shape=(
            jax.ShapeDtypeStruct((m, length // m, hc), bf16),
            jax.ShapeDtypeStruct((length, cc), f32),
            jax.ShapeDtypeStruct((8, length), f32),
        ),
        in_specs=[vmem] * len(args),
        out_specs=(vmem,) * 3,
        scratch_shapes=[
            pltpu.VMEM((length, args[2].shape[1]), f32),
            pltpu.VMEM((2, length, rank), bf16),
            pltpu.VMEM((length + 2 * top, cc), f32),
            pltpu.VMEM((2, chunks, GROUP, GROUP), f32),
            pltpu.VMEM((2, chunks, GROUP, GROUP), f32),
            pltpu.VMEM((2, length, GROUP), f32),
            pltpu.VMEM((2, length, GROUP), f32),
            pltpu.VMEM((2, chunks, GROUP, GROUP), f32),
        ],
    )(*args)


def output_kernel(
    n, m, hc, cc, pack,
    mix_ref, conv_ref, sums_ref, cs_ref, wm_ref, wc_ref, out_ref,
    own, around, mates_act, sums_in, wm_in, wc_in, total, block,
    local, ssend, srecv, vsend, vrecv, asend, arecv, dsend, drecv, osend, orecv,
):
    s, t = lax.axis_index("sp"), lax.axis_index("tp")
    here = s * m + t
    everyone = n * m
    length = conv_ref.shape[0]
    half = length // m
    share = half // n
    columns = wm_ref.shape[1]
    packed = half // pack
    mates = [lax.rem(t + k, m) for k in range(1, m)]

    def other(k):
        p = lax.rem(here + k, everyone)
        return {"sp": p // m, "tp": p % m}

    greet([other(k) for k in range(1, everyone)])
    outs = []
    for k in range(1, everyone):
        outs.append(remote(sums_ref, sums_in.at[k - 1], ssend.at[k - 1], srecv.at[k - 1], other(k)))
    for j in range(m - 1):
        outs.append(remote(wm_ref, wm_in.at[j], vsend.at[0, j], vrecv.at[0, j], {"tp": mates[j]}))
        outs.append(remote(wc_ref, wc_in.at[j], vsend.at[1, j], vrecv.at[1, j], {"tp": mates[j]}))
    for copy in outs:
        copy.start()
    width = mix_ref.shape[2]
    for c in range(m):
        for i in range(pack):
            own[c, pl.ds(0, packed), pl.ds(i * hc, hc)] = mix_ref[c, pl.ds(i * packed, packed), :]
    pieces = m + 1

    def slab(ref, i):
        if i == 0:
            return ref.at[:, pl.ds(0, packed)]
        return ref.at[lax.rem(t + i, m), pl.ds(packed, half)]

    def along(k, way, i):
        b = s - k if way == 0 else s + k
        src = slab(own if k == 0 else around.at[b], i)
        return remote(
            src, slab(around.at[b], i), asend.at[way, k, i], arecv.at[way, k, i], {"sp": s + 1 if way == 0 else s - 1}
        )

    def sends(k, way):
        return (s - k >= 0) & (s < n - 1) if way == 0 else (s + k < n) & (s > 0)

    def gets(k, way):
        return s - 1 - k >= 0 if way == 0 else s + 1 + k < n

    def across(index, j, b, i):
        at = pl.ds(0, packed) if i == 0 else pl.ds(packed, half)
        src = own.at[mates[j], at] if index == 0 else around.at[b, mates[j], at]
        return remote(src, mates_act.at[j, b, at], dsend.at[index, j, i], drecv.at[index, j, i], {"tp": mates[j]})

    def add(b, act, wm, wc):
        w = wm[pl.ds(pl.multiple_of(b * hc, hc), hc), :]
        for i in range(pack):
            rows = pl.ds(i * packed, packed)
            total[rows, :] += dot1(act[pl.ds(0, packed), pl.ds(i * hc, hc)], w)
        total[...] += dot1(act[pl.ds(packed, half), :], wc[pl.ds(pl.multiple_of(b * cc, cc), cc), :])

    def pass_on(k, i):
        for way in range(2):
            @pl.when(gets(k, way))
            def _():
                b = s - 1 - k if way == 0 else s + 1 + k
                part = slab(around.at[b], i)
                remote(part, part, asend.at[way, k, i], arecv.at[way, k, i], {"sp": b}).wait_recv()
                if k + 1 < n - 1:
                    @pl.when(sends(k + 1, way))
                    def _():
                        along(k + 1, way, i).start()
                if i == 0:
                    for j in range(m - 1):
                        across(1 + 2 * k + way, j, b, 0).start()
                elif i < m:
                    across(1 + 2 * k + way, i - 1, b, 1).start()

    def begin(i):
        for way in range(2):
            @pl.when(sends(0, way))
            def _():
                along(0, way, i).start()

    begin(0)
    for j in range(m - 1):
        across(0, j, s, 0).start()
    for copy in outs[: everyone - 1]:
        copy.wait()
    stats = sums_ref[...]
    for k in range(everyone - 1):
        stats += sums_in[k]
    row = lax.broadcasted_iota(jnp.int32, (8, cc), 0)
    channels = cc * n * m

    def spread(which):
        return lax.dot_general(
            stats, (row == which).astype(f32), TN, precision=lax.Precision.HIGHEST, preferred_element_type=f32
        )

    mean = spread(0) / channels
    power = spread(1) / channels - mean * mean
    gain = pick(cs_ref, s, n, cc)
    done = jax.nn.silu((conv_ref[...] - mean) * lax.rsqrt(power + 1e-05) * gain).astype(bf16)
    for token in range(0, length, share):
        unit = token // share
        own[unit % m, pl.ds(packed + (unit // m) * share, share), :] = done[token : token + share]

    for i in range(1, pieces):
        begin(i)
    for j in range(m - 1):
        across(0, j, s, 1).start()
    total[...] = jnp.zeros_like(total)
    pass_on(0, 0)
    add(s, own.at[t], wm_ref, wc_ref)
    for copy in outs[everyone - 1 :]:
        copy.wait()

    def from_mates(index, b):
        for j in range(m - 1):
            for i in range(2):
                across(index, j, b, i).wait_recv()
            add(b, mates_act.at[j, b], wm_in.at[j], wc_in.at[j])
            for i in range(2):
                across(index, j, b, i).wait_send()

    for k in range(n - 1):
        if k > 0:
            pass_on(k, 0)
        for i in range(1, pieces):
            pass_on(k, i)
        for way in range(2):
            @pl.when(gets(k, way))
            def _():
                b = s - 1 - k if way == 0 else s + 1 + k
                add(b, around.at[b, t], wm_ref, wc_ref)
        if k == 0:
            from_mates(0, s)
        else:
            for way in range(2):
                @pl.when(gets(k - 1, way))
                def _():
                    from_mates(2 * k - 1 + way, s - k if way == 0 else s + k)
    for way in range(2):
        @pl.when(gets(n - 2, way))
        def _():
            from_mates(2 * n - 3 + way, s - n + 1 if way == 0 else s + n - 1)
    for k in range(n - 1):
        for way in range(2):
            @pl.when(sends(k, way))
            def _():
                for i in range(pieces):
                    along(k, way, i).wait_send()
    block[...] = total[...].astype(bf16)
    mine = out_ref.at[:, pl.ds(pl.multiple_of(s * columns, columns), columns)]
    keep = pltpu.make_async_copy(block.at[pl.ds(s * share, share)], mine, local.at[0])
    keep.start()
    final = []
    for k in range(1, n):
        p = lax.rem(s + k, n)
        copy = remote(block.at[pl.ds(p * share, share)], mine, osend.at[k - 1], orecv.at[k - 1], {"sp": p})
        copy.start()
        final.append(copy)
    for k in range(1, n):
        p = lax.rem(s + n - k, n)
        part = out_ref.at[:, pl.ds(pl.multiple_of(p * columns, columns), columns)]
        remote(part, part, osend.at[k - 1], orecv.at[k - 1], {"sp": p}).wait_recv()
        final[k - 1].wait_send()
    keep.wait()


def output(n, m, hc, cc, mixed, conv, sums, cs, wm, wc):
    length = conv.shape[0]
    half, columns = length // m, wm.shape[1]
    pack = max(cc // hc, 1)
    rows = half // pack + half
    vmem = pl.BlockSpec(memory_space=pltpu.VMEM)
    dma = pltpu.SemaphoreType.DMA
    hops, mates = max(n - 1, 1), max(m - 1, 1)
    return pl.pallas_call(
        functools.partial(output_kernel, n, m, hc, cc, pack),
        out_shape=jax.ShapeDtypeStruct((half // n, n * columns), bf16),
        in_specs=[vmem] * 6,
        out_specs=vmem,
        scratch_shapes=[
            pltpu.VMEM((m, rows, cc), bf16),
            pltpu.VMEM((n, m, rows, cc), bf16),
            pltpu.VMEM((mates, n, rows, cc), bf16),
            pltpu.VMEM((n * m - 1, 8, length), f32),
            pltpu.VMEM((mates,) + wm.shape, bf16),
            pltpu.VMEM((mates,) + wc.shape, bf16),
            pltpu.VMEM((half, columns), f32),
            pltpu.VMEM((half, columns), bf16),
            dma((1,)),
            dma((n * m - 1,)), dma((n * m - 1,)),
            dma((2, mates)), dma((2, mates)),
            dma((2, hops, m + 1)), dma((2, hops, m + 1)),
            dma((2 * n - 1, mates, 2)), dma((2 * n - 1, mates, 2)),
            dma((hops,)), dma((hops,)),
        ],
        compiler_params=pltpu.CompilerParams(collective_id=1, has_side_effects=True),
    )(mixed, conv, sums, cs, wm, wc)


highest = lax.Precision.HIGHEST


def carried_in(x, axis, combine, identity, reverse):
    length, here = (lax.axis_size(axis), lax.axis_index(axis))
    everything = jax.tree.map(
        lambda part, kind: lax.all_gather(part.astype(kind), axis), x, (jnp.bfloat16, jnp.bfloat16)
    )
    start = jax.tree.map(
        lambda part, zero: jnp.broadcast_to(jnp.asarray(zero, part.dtype), part.shape), x, identity
    )

    def hop(k, before):
        at = length - 1 - k if reverse else k
        reached = at > here if reverse else at < here
        new = combine(
            before, jax.tree.map(lambda part, own: part[at].astype(own.dtype), everything, x)
        )
        return jax.tree.map(lambda a, b: jnp.where(reached, a, b), new, before)

    return lax.fori_loop(0, length, hop, start)


def padded_2(block, sides, width):
    for axis, dim in sides:
        count = lax.axis_size(axis)
        forward = [(i, i + 1) for i in range(count - 1)]
        backward = [(target, source) for source, target in forward]
        low = lax.ppermute(
            lax.slice_in_dim(block, block.shape[dim] - width, None, axis=dim), axis, forward
        )
        high = lax.ppermute(lax.slice_in_dim(block, 0, width, axis=dim), axis, backward)
        block = jnp.concatenate([low, block, high], axis=dim)
    return block


def split_heads(values):
    return values.reshape(values.shape[0], -1, GROUP)


def paired(values):
    return jnp.stack([values, jnp.flip(values, 0)], 1)


def local_step(stacked, inputs):
    fading_multiplier, unit_key, rated_key, keys, values, query = inputs
    projected = jnp.einsum("dhvk,dhk->dhv", stacked, unit_key, precision=highest)
    outer = values[..., None] * keys[:, :, None, :]
    added = jnp.concatenate([jnp.zeros_like(outer), outer], axis=2)
    stacked = (
        stacked * fading_multiplier[:, :, None, :]
        - projected[..., None] * rated_key[:, :, None, :]
        + added
    )
    return (stacked, jnp.einsum("dhvk,dhk->dhv", stacked, query, precision=highest))


def chain_pair(earlier, later):
    product = jnp.einsum("hij,hjk->hik", earlier[0], later[0], precision=highest)
    moved = jnp.einsum("hij,hjk->hik", earlier[1], later[0], precision=highest) + later[1]
    return (product, moved)


def carry_in(initial_memory_matrix, prefix):
    return (
        jnp.einsum("hij,hjk->hik", initial_memory_matrix, prefix[0], precision=highest) + prefix[1]
    )


def head_norm(summed, head_norm_scale):
    centered = summed - jnp.mean(summed, axis=-1, keepdims=True)
    scaled = centered * lax.rsqrt(jnp.mean(centered * centered, axis=-1, keepdims=True) + 0.00064)
    return (
        (scaled * head_norm_scale.reshape(-1, GROUP))
        .reshape(summed.shape[0], -1)
        .astype(jnp.bfloat16)
    )


def rounded(total):
    return lax.optimization_barrier(total.astype(jnp.bfloat16)).astype(jnp.float32)


def mixer_branch(
    normed,
    sums,
    decay_down_weight,
    decay_up_weight,
    decay_bias_base,
    decay_position_offset,
    extra_log_decay,
    correction_down_weight,
    correction_up_weight,
    correction_rate_bias,
    head_norm_scale,
    starting_states,
):
    query = rounded(sums[0])
    keys = rounded(sums[1])
    values = rounded(sums[2])
    low_decay = jnp.tanh(
        jnp.dot(normed, decay_down_weight, preferred_element_type=jnp.float32)
    ).astype(jnp.bfloat16)
    fading_raw_scores = (
        decay_bias_base
        + jnp.dot(low_decay, decay_up_weight, preferred_element_type=jnp.float32)
        + jnp.repeat(decay_position_offset[0], GROUP, axis=1)
    )
    fading_multiplier = jnp.exp(
        -jnp.exp(-jax.nn.softplus(-fading_raw_scores) - 0.5)
        + jnp.repeat(extra_log_decay[0], GROUP, axis=1)
    )
    low_rate = jnp.dot(normed, correction_down_weight, preferred_element_type=jnp.float32).astype(
        jnp.bfloat16
    )
    rate = jax.nn.sigmoid(
        correction_rate_bias
        + jnp.dot(low_rate, correction_up_weight, preferred_element_type=jnp.float32)
    )
    key_heads = split_heads(keys)
    unit_key = key_heads * lax.rsqrt(jnp.sum(key_heads * key_heads, axis=-1, keepdims=True) + 1e-06)
    rated_key = unit_key * split_heads(rate)
    steps = tuple(
        (
            paired(item)
            for item in (
                split_heads(fading_multiplier),
                unit_key,
                rated_key,
                key_heads,
                split_heads(values),
                split_heads(query),
            )
        )
    )
    heads_here = key_heads.shape[1]
    identity = jnp.broadcast_to(
        jnp.eye(GROUP, dtype=jnp.float32),
        (2, heads_here, GROUP, GROUP),
    )
    nothing = jnp.zeros((2, heads_here, GROUP, GROUP), jnp.float32)
    start = jnp.concatenate([identity, nothing], axis=2)
    ends, emitted = lax.scan(local_step, start, steps, unroll=8)
    transfer = ends[:, :, :GROUP]
    alone = ends[:, :, GROUP:]
    through = emitted[..., :GROUP]
    own_part = emitted[..., GROUP:]
    before = carried_in((transfer[0], alone[0]), "sp", chain_pair, (identity[0], nothing[0]), False)
    after = carried_in((transfer[1], alone[1]), "sp", chain_pair, (identity[1], nothing[1]), True)
    starts = jnp.stack(
        [carry_in(starting_states[0, 0], before), carry_in(starting_states[0, 1], after)], 0
    )
    outputs = jnp.einsum("dhvk,tdhk->tdhv", starts, through, precision=highest) + own_part
    summed = outputs[:, 0] + jnp.flip(outputs[:, 1], 0)
    return head_norm(summed, head_norm_scale)


def conv_branch(sums, depthwise_taps_weight, channel_norm_scale):
    glu = (sums[0] * jax.nn.sigmoid(sums[1])).astype(jnp.bfloat16)
    reach = depthwise_taps_weight.shape[0] // 2
    padded = padded_2(glu, (("sp", 0),), reach)
    conv = lax.conv_general_dilated(
        padded.astype(jnp.float32)[None],
        depthwise_taps_weight[:, None, :],
        (1,),
        "VALID",
        dimension_numbers=("NWC", "WIO", "NWC"),
        feature_group_count=depthwise_taps_weight.shape[1],
        precision=highest,
    )[0]
    first, second = lax.psum((jnp.sum(conv, axis=-1), jnp.sum(conv * conv, axis=-1)), "tp")
    width = conv.shape[1] * lax.axis_size("tp")
    mean = first / width
    power = second / width - mean * mean
    return jax.nn.silu(
        (conv - mean[:, None]) * lax.rsqrt(power[:, None] + 1e-05) * channel_norm_scale
    ).astype(jnp.bfloat16)


def spread_device(
    inputs,
    input_norm_scale,
    query_matrix,
    key_matrix,
    value_matrix,
    decay_down_weight,
    decay_up_weight,
    decay_bias_base,
    decay_position_offset,
    extra_log_decay,
    correction_down_weight,
    correction_up_weight,
    correction_rate_bias,
    head_norm_scale,
    starting_states,
    pointwise_value_weight,
    pointwise_gate_weight,
    depthwise_taps_weight,
    channel_norm_scale,
    mixer_output_weight,
    convolution_output_weight,
):
    symbol_vectors = lax.all_gather(inputs[0], "tp", axis=1, tiled=True)
    as_float = symbol_vectors.astype(jnp.float32)
    normed = (
        as_float
        * lax.rsqrt(jnp.mean(as_float * as_float, axis=-1, keepdims=True) + 1e-06)
        * input_norm_scale
    ).astype(jnp.bfloat16)
    mixer_args = (
        decay_down_weight,
        decay_up_weight,
        decay_bias_base,
        decay_position_offset,
        extra_log_decay,
        correction_down_weight,
        correction_up_weight,
        correction_rate_bias,
        head_norm_scale,
        starting_states,
    )
    pieces = (
        lax.all_gather(query_matrix, "sp", axis=0, tiled=True),
        lax.all_gather(key_matrix, "sp", axis=0, tiled=True),
        lax.all_gather(value_matrix, "sp", axis=0, tiled=True),
        lax.all_gather(pointwise_value_weight, "sp", axis=0, tiled=True),
        lax.all_gather(pointwise_gate_weight, "sp", axis=0, tiled=True),
    )
    sums = tuple((jnp.dot(normed, piece, preferred_element_type=jnp.float32) for piece in pieces))
    mixer_out = mixer_branch(normed, sums[:3], *mixer_args)
    conv_out = conv_branch(sums[3:], depthwise_taps_weight, channel_norm_scale)
    joined = jnp.concatenate([mixer_out, conv_out], axis=1)
    weight_rows = jnp.concatenate([mixer_output_weight, convolution_output_weight], axis=0)
    columns = lax.all_gather(weight_rows, "sp", axis=1, tiled=True)
    moved = lax.all_to_all(joined, "tp", split_axis=0, concat_axis=1, tiled=True)
    every_row = lax.all_gather(columns, "tp", axis=0, tiled=True)
    total = jnp.dot(moved, every_row, preferred_element_type=jnp.float32)
    return total.astype(jnp.bfloat16)[None]


def per_device(
    inputs, input_norm_scale, query_matrix, key_matrix, value_matrix,
    decay_down_weight, decay_up_weight, decay_bias_base, decay_position_offset, extra_log_decay,
    correction_down_weight, correction_up_weight, correction_rate_bias, head_norm_scale, starting_states,
    pointwise_value_weight, pointwise_gate_weight, depthwise_taps_weight, channel_norm_scale,
    mixer_output_weight, convolution_output_weight,
):
    n, m, nf = lax.axis_size("sp"), lax.axis_size("tp"), lax.axis_size("fs")
    lanes = query_matrix.shape[1] % (n * GROUP) or pointwise_value_weight.shape[1] % (n * 128)
    if lanes or query_matrix.shape[0] % (nf * 16):
        return spread_device(
            inputs, input_norm_scale, query_matrix, key_matrix, value_matrix,
            decay_down_weight, decay_up_weight, decay_bias_base, decay_position_offset, extra_log_decay,
            correction_down_weight, correction_up_weight, correction_rate_bias, head_norm_scale, starting_states,
            pointwise_value_weight, pointwise_gate_weight, depthwise_taps_weight, channel_norm_scale,
            mixer_output_weight, convolution_output_weight,
        )
    x = inputs[0]
    rows = x.shape[0]
    hc, cc = query_matrix.shape[1] // n, pointwise_value_weight.shape[1] // n
    parts = [query_matrix, key_matrix, pointwise_value_weight, pointwise_gate_weight, value_matrix]
    e = jnp.concatenate([decay_position_offset[0], extra_log_decay[0]], axis=1).T
    everything, columns, shifts = collect(n, m, nf, x, parts, e)
    mixed, conv, sums = mix(
        n, m, hc, cc, rows,
        everything, input_norm_scale[None], columns, shifts,
        decay_down_weight, decay_up_weight, decay_bias_base[None],
        correction_down_weight, correction_up_weight, correction_rate_bias[None],
        head_norm_scale[None], starting_states, depthwise_taps_weight,
    )
    return output(
        n, m, hc, cc, mixed, conv, sums, channel_norm_scale[None], mixer_output_weight, convolution_output_weight
    )[None]


def solution(mesh):
    return jax.shard_map(
        per_device,
        mesh=mesh,
        in_specs=(
            P("fs", "sp", "tp"),
            P(),
            P("sp", "tp"),
            P("sp", "tp"),
            P("sp", "tp"),
            P(),
            P(None, "tp"),
            P("tp"),
            P("fs", "sp", "tp"),
            P("fs", "sp", "tp"),
            P(),
            P(None, "tp"),
            P("tp"),
            P("tp"),
            P("fs", None, "tp", None, None),
            P("sp", "tp"),
            P("sp", "tp"),
            P(None, "tp"),
            P("tp"),
            P("tp", "sp"),
            P("tp", "sp"),
        ),
        out_specs=P("fs", ("sp", "tp"), None),
        check_vma=False,
    )
```
